512 devices in a mesh: ep: 32 (over z, core), tp: 16 (over y, x).
Axes of the slice: x: 4, y: 4, z: 16, core: 2. Of those that a mesh axis runs over, the one named last changes fastest.
Arguments:
- query_vectors: bfloat16 [16384, 4096], P('ep', 'tp'), may hold values from -6 to 6
- key_vectors: bfloat16 [16384, 2048], P('ep', 'tp'), may hold values from -6 to 6
- value_vectors: bfloat16 [16384, 2048], P('ep', 'tp'), may hold values from -64 to 64
- query_gain: float32 [128], replicated, may hold values from 0.1 to 1.9
- key_gain: float32 [128], replicated, may hold values from 0.1 to 1.9
- sink_logits: float32 [32], P('tp'), may hold values from 3 to 7
- moe_rows: bfloat16 [5120, 4096], P('ep', 'tp'), may hold values from -6 to 6
- norm_gain: float32 [4096], replicated, may hold values from 0.1 to 1.9
- expert_ids: int32 [5120, 4], P('ep'), may hold values from 0 to 31, all different within a row; in each aligned block of 160 rows (0 to 159, 160 to 319, ...) at most 30 rows name the same one
- route_weights: float32 [5120, 4], P('ep'), may hold values from 0.25 to 2.5
- expert_gate: bfloat16 [32, 4096, 2048], P('ep', None, 'tp'), may hold values from -0.09375 to 0.09375
- expert_up: bfloat16 [32, 4096, 2048], P('ep', None, 'tp'), may hold values from -0.09375 to 0.09375
- expert_down: bfloat16 [32, 2048, 4096], P('ep', None, 'tp'), may hold values from -0.125 to 0.125
- shared_gate: bfloat16 [4096, 512], P(None, 'tp'), may hold values from -0.09375 to 0.09375
- shared_up: bfloat16 [4096, 512], P(None, 'tp'), may hold values from -0.09375 to 0.09375
- shared_down: bfloat16 [512, 4096], P(None, 'tp'), may hold values from -0.25 to 0.25
Outputs:
- attended: bfloat16 [16384, 4096], P('ep', 'tp')
- moe_out: bfloat16 [5120, 4096], P('ep', 'tp')
The draws below stay inside these ranges and needn't reach their ends.
Inputs may be any that keep to these rules, and one draw needn't show every extreme that they name: `expert_ids`: each row names 4 different experts. Within the rows of one index of ep (aligned blocks of 160 rows), no expert is named by more than 30 rows, and in some block one expert is named by exactly 30.
All inputs are finite; a program needn't handle non-finite values.
Results may differ from the reference program's by a relative error of at most 0.0071.
Values may be sent and summed in bfloat16 or wider, within the bound.
A program may use at most 64 MiB of HBM per device.

```python
import math
import jax
import jax.numpy as jnp
import numpy as np
from jax import lax

HEAD_DIM = 128
HEADS = 32
KV_HEADS = 16
GROUP = 2
WINDOW = 128
GRID_W = 64
TOK_A = 512
SEQ_A = 16384
D = 4096
F = 2048
FS = 512
TOP_K = 4
TOK_B = 160
TOKENS_B = 5120
EXPERTS = 32
CAP = 30


def levels(stream_key, shape, shards, least, largest):
    def one(position, parts):
        steps = jax.random.uniform(jax.random.fold_in(jax.random.fold_in(stream_key, 6), position), (parts,), jnp.float32, least / len(shards), largest / len(shards))
        return jnp.repeat(jnp.exp(steps), shape[position] // parts).reshape((-1,) + (1,) * (len(shape) - position - 1))

    loudness = one(*shards[0])
    for cut in shards[1:]:
        loudness = loudness * one(*cut)
    return loudness


def shared_out(key, own, number, rows, number_of, top, bound, lean):
    sequence = jax.random.permutation(key, number_of)
    heavy_load, ordinary = portions_of(number_of, rows * top, bound, lean, True), portions_of(number_of, rows * top, bound, lean, False)
    places = jnp.arange(number_of)

    def named(sizes, offset_by):
        used = int((sizes > 0).sum())
        fixed = max(1, used // 4)
        shifted = fixed + (places - fixed + offset_by * (used - fixed)) % max(1, number_of - fixed)
        return jnp.zeros((number_of,), jnp.int32).at[sequence[jnp.where(places < fixed, places, shifted)]].set(jnp.asarray(sizes, jnp.int32))

    sizes = jnp.where(number % 4 == 0, named(heavy_load, number // 4), named(ordinary, number - number // 4 - 1))
    mixed = jax.random.permutation(jax.random.fold_in(own, 3), number_of)
    giver, receiver = mixed[0:number_of // 2 * 2:2], mixed[1:number_of // 2 * 2:2]
    room = jnp.minimum(sizes[giver] - 1, bound - sizes[receiver]) // 2
    room = jnp.where((giver == sequence[0]) | (receiver == sequence[0]) | (sizes[receiver] == 0), 0, jnp.maximum(room, 0))
    shifted = jax.random.randint(jax.random.fold_in(own, 4), (number_of // 2,), 0, 1 << 20) % (room + 1)
    sizes = sizes.at[giver].add(-shifted).at[receiver].add(shifted)
    items = jnp.searchsorted(jnp.cumsum(sizes), jnp.arange(rows * top), side="right").astype(jnp.int32)
    table = items.reshape(top, rows).T
    table = table[jax.random.permutation(jax.random.fold_in(own, 1), rows)]
    offset_by = jax.random.randint(jax.random.fold_in(own, 2), (rows, 1), 0, top)
    return jnp.take_along_axis(table, (jnp.arange(top)[None, :] + offset_by) % top, axis=1)


def portions_of(amount, total, most, skew, full):
    portions = [(1 << 20) // math.isqrt(standing ** skew) + 1 for standing in range(1, amount + 1)]
    largest = most if full else min(most, max(-(-total // amount), total * portions[0] // sum(portions)))
    least = 1 if total - largest >= amount - 1 else 0
    holding, rest = [largest] + [least] * (amount - 1), total - largest - least * (amount - 1)
    while rest > 0:
        free = [i for i in range(1, amount) if holding[i] < largest] or [i for i in range(1, amount) if holding[i] < most]
        pool, budget = sum([portions[i] for i in free]), rest
        for i in free:
            extra = min(most - holding[i], max(1, budget * portions[i] // pool), rest)
            holding[i] = holding[i] + extra
            rest = rest - extra
    return np.array(holding)


def gaussian(own_key, shape, width, reach, cuts=(), kind=jnp.bfloat16):
    result = width * jax.random.normal(own_key, shape, jnp.float32)
    if cuts:
        result = result * levels(own_key, shape, cuts, -0.22, 0.18)
    return jnp.clip(result, -reach, reach).astype(kind)


def setup_inputs(seed: int = 0) -> dict:
    seeds = jax.random.split(jax.random.key(seed), 17)
    query_vectors = gaussian(seeds[0], (SEQ_A, HEADS * HEAD_DIM), 1.0, 6.0, ((0, 32), (1, 16)))
    key_vectors = gaussian(seeds[1], (SEQ_A, KV_HEADS * HEAD_DIM), 1.0, 6.0, ((0, 32), (1, 16)))
    value_vectors = gaussian(seeds[2], (SEQ_A, KV_HEADS * HEAD_DIM), 12.0, 64.0, ((0, 32), (1, 16)))
    query_gain = jnp.clip(1.0 + 0.18 * jax.random.normal(seeds[3], (HEAD_DIM,), jnp.float32), 0.1, 1.9)
    key_gain = jnp.clip(1.0 + 0.18 * jax.random.normal(seeds[4], (HEAD_DIM,), jnp.float32), 0.1, 1.9)
    sink_logits = jnp.clip(3.0 + 4.0 * jax.random.uniform(seeds[5], (HEADS,), jnp.float32) ** levels(seeds[5], (HEADS,), ((0, 16),), -0.2, 0.2), 3.0, 7.0)
    moe_rows = gaussian(seeds[6], (TOKENS_B, D), 1.0, 6.0, ((0, 32), (1, 16)))
    norm_gain = jnp.clip(1.0 + 0.18 * jax.random.normal(seeds[7], (D,), jnp.float32), 0.1, 1.9)
    expert_ids_keys = jax.random.split(jax.random.fold_in(seeds[8], 1), TOKENS_B // TOK_B)
    expert_ids_turns = jax.random.permutation(jax.random.fold_in(seeds[8], 3), TOKENS_B // TOK_B)
    expert_ids = jax.vmap(lambda own, number: shared_out(jax.random.fold_in(seeds[8], 2), own, number, TOK_B, EXPERTS, TOP_K, CAP, 2))(expert_ids_keys, expert_ids_turns).reshape((TOKENS_B, TOP_K))
    route_weights = jnp.clip(jnp.exp(math.log(2.5) - 2.3025851 * jax.random.uniform(seeds[9], (TOKENS_B, TOP_K), jnp.float32) ** levels(seeds[9], (TOKENS_B, TOP_K), ((0, 32),), -0.2, 0.2)), 0.25, 2.5)
    expert_gate = gaussian(seeds[10], (EXPERTS, D, F), D ** -0.5, 0.09375, ((0, 32), (2, 16)))
    expert_up = gaussian(seeds[11], (EXPERTS, D, F), D ** -0.5, 0.09375, ((0, 32), (2, 16)))
    expert_down = gaussian(seeds[12], (EXPERTS, F, D), F ** -0.5, 0.125, ((0, 32), (2, 16)))
    shared_gate = gaussian(seeds[13], (D, FS), D ** -0.5, 0.09375, ((1, 16),))
    shared_up = gaussian(seeds[14], (D, FS), D ** -0.5, 0.09375, ((1, 16),))
    shared_down = gaussian(seeds[15], (FS, D), FS ** -0.5, 0.25, ((1, 16),))
    return dict(query_vectors=query_vectors, key_vectors=key_vectors, value_vectors=value_vectors, query_gain=query_gain, key_gain=key_gain, sink_logits=sink_logits, moe_rows=moe_rows, norm_gain=norm_gain, expert_ids=expert_ids, route_weights=route_weights, expert_gate=expert_gate, expert_up=expert_up, expert_down=expert_down, shared_gate=shared_gate, shared_up=shared_up, shared_down=shared_down)


epsilon = 1e-06
rotary_base = 10000.0

def half_turn(halves):
    leading, trailing = jnp.split(halves, 2, axis=-1)
    return jnp.concatenate([-trailing, leading], axis=-1)

def rotate_heads(vectors, head_gain, positions):
    floats = vectors.astype(jnp.float32)
    normed = floats * lax.rsqrt(lax.optimization_barrier(jnp.mean(floats * floats, axis=-1, keepdims=True)) + epsilon) * head_gain
    quarter = HEAD_DIM // 4
    freq_index = jnp.arange(quarter, dtype=jnp.int32).astype(jnp.float32)
    inverse = rotary_base ** (-4.0 * freq_index / HEAD_DIM)
    grid_row = (positions // GRID_W).astype(jnp.float32)[:, None] * inverse
    grid_col = (positions % GRID_W).astype(jnp.float32)[:, None] * inverse
    angles = jnp.concatenate([grid_row, grid_row, grid_col, grid_col], axis=-1)[:, None, :]
    row_half, col_half = jnp.split(normed, 2, axis=-1)
    turned = jnp.concatenate([half_turn(row_half), half_turn(col_half)], axis=-1)
    return (normed * jnp.cos(angles) + turned * jnp.sin(angles)).astype(jnp.bfloat16)

def activate(block_rows, gate_weight, up_weight, factor):
    gate_sum = jnp.dot(block_rows, gate_weight, preferred_element_type=jnp.float32) * factor[:, None]
    up_sum = jnp.dot(block_rows, up_weight, preferred_element_type=jnp.float32) * factor[:, None]
    return (jax.nn.silu(gate_sum) * up_sum).astype(jnp.bfloat16)

def windowed(query_vectors, key_vectors, value_vectors, query_gain, key_gain, sink_logits):
    positions = jnp.arange(SEQ_A, dtype=jnp.int32)
    queries = rotate_heads(query_vectors.reshape(SEQ_A, HEADS, HEAD_DIM), query_gain, positions)
    turned_keys = rotate_heads(key_vectors.reshape(SEQ_A, KV_HEADS, HEAD_DIM), key_gain, positions)
    values = value_vectors.reshape(SEQ_A, KV_HEADS, HEAD_DIM)
    padding = ((WINDOW, WINDOW), (0, 0), (0, 0))
    padded_keys = jnp.pad(turned_keys, padding)
    padded_values = jnp.pad(values, padding)
    blocks = SEQ_A // TOK_A
    query_blocks = queries.reshape(blocks, TOK_A, KV_HEADS, GROUP, HEAD_DIM)
    sink_scale = jnp.exp(sink_logits).reshape(KV_HEADS, GROUP)
    extent = TOK_A + 2 * WINDOW
    score_scale = HEAD_DIM ** (-0.5)

    def attend_block(packed):
        query_block, block_index = packed
        first_row = (block_index * TOK_A).astype(jnp.int32)
        near_keys = lax.dynamic_slice_in_dim(padded_keys, first_row, extent, 0)
        near_values = lax.dynamic_slice_in_dim(padded_values, first_row, extent, 0)
        query_pos = first_row + jnp.arange(TOK_A, dtype=jnp.int32)
        key_pos = first_row - WINDOW + jnp.arange(extent, dtype=jnp.int32)
        inside = (jnp.abs(query_pos[:, None] - key_pos[None, :]) <= WINDOW) & (key_pos >= 0)[None, :] & (key_pos < SEQ_A)[None, :]
        scores = jnp.einsum('qhgd,khd->hgqk', query_block.astype(jnp.float32), near_keys.astype(jnp.float32)) * score_scale
        raised = jnp.where(inside, jnp.exp(scores), 0.0)
        denominator = sink_scale[:, :, None] + lax.optimization_barrier(jnp.sum(raised, axis=-1))
        weights = (raised / denominator[..., None]).astype(jnp.bfloat16)
        mixed = jnp.einsum('hgqk,khd->qhgd', weights.astype(jnp.float32), near_values.astype(jnp.float32))
        return mixed.astype(jnp.bfloat16).reshape(TOK_A, HEADS * HEAD_DIM)
    outputs = lax.map(attend_block, (query_blocks, jnp.arange(blocks, dtype=jnp.int32)))
    return outputs.reshape(SEQ_A, HEADS * HEAD_DIM)

def moe_layer(moe_rows, norm_gain, expert_ids, route_weights, expert_gate, expert_up, expert_down, shared_gate, shared_up, shared_down):
    floats = moe_rows.astype(jnp.float32)
    inverse_rms = lax.rsqrt(lax.optimization_barrier(jnp.mean(floats * floats, axis=-1)) + epsilon)
    scaled = (floats * norm_gain).astype(jnp.bfloat16)
    shared_hidden = activate(scaled, shared_gate, shared_up, inverse_rms)
    shared_result = jnp.dot(shared_hidden, shared_down, preferred_element_type=jnp.float32)
    blocks = TOKENS_B // TOK_B
    flat_ids = expert_ids.reshape(blocks, TOK_B * TOP_K).astype(jnp.int32)
    onehot = (flat_ids[:, :, None] == jnp.arange(EXPERTS, dtype=jnp.int32)[None, None, :]).astype(jnp.int32)
    slot_index = lax.optimization_barrier(jnp.sum((jnp.cumsum(onehot, axis=1) - onehot) * onehot, axis=-1)).astype(jnp.int32)
    owner_row = jnp.arange(TOK_B * TOP_K, dtype=jnp.int32) // TOP_K
    scaled_blocks = scaled.reshape(blocks, TOK_B, D)
    rms_blocks = inverse_rms.reshape(blocks, TOK_B)
    capacity_index = jnp.arange(CAP, dtype=jnp.int32)

    def one_expert(packed):
        expert, gate_weight, up_weight, down_weight = packed
        matches = (flat_ids == expert)[:, :, None] & (slot_index[:, :, None] == capacity_index[None, None, :])
        present = jnp.any(matches, axis=1)
        source_row = lax.optimization_barrier(jnp.sum(jnp.where(matches, owner_row[None, :, None], 0), axis=1)).astype(jnp.int32)
        picked = jnp.take_along_axis(scaled_blocks, source_row[:, :, None], axis=1)
        picked = jnp.where(present[:, :, None], picked, jnp.zeros((), jnp.bfloat16))
        factor = jnp.where(present, jnp.take_along_axis(rms_blocks, source_row, axis=1), 0.0)
        hidden = activate(picked.reshape(blocks * CAP, D), gate_weight, up_weight, factor.reshape(blocks * CAP))
        return jnp.dot(hidden, down_weight, preferred_element_type=jnp.float32).astype(jnp.bfloat16).reshape(blocks, CAP, D)
    results = lax.map(one_expert, (jnp.arange(EXPERTS, dtype=jnp.int32), expert_gate, expert_up, expert_down))
    block_ids = expert_ids.reshape(blocks, TOK_B, TOP_K).astype(jnp.int32)
    block_slots = slot_index.reshape(blocks, TOK_B, TOP_K)
    source_block = jnp.arange(blocks, dtype=jnp.int32)[:, None, None]
    gathered = results[block_ids, source_block, block_slots]
    routed = lax.optimization_barrier(jnp.sum(route_weights.reshape(blocks, TOK_B, TOP_K, 1) * gathered.astype(jnp.float32), axis=2))
    return (shared_result + routed.reshape(TOKENS_B, D)).astype(jnp.bfloat16)

def reference(query_vectors, key_vectors, value_vectors, query_gain, key_gain, sink_logits, moe_rows, norm_gain, expert_ids, route_weights, expert_gate, expert_up, expert_down, shared_gate, shared_up, shared_down):
    attended = windowed(query_vectors, key_vectors, value_vectors, query_gain, key_gain, sink_logits)
    moe_out = moe_layer(moe_rows, norm_gain, expert_ids, route_weights, expert_gate, expert_up, expert_down, shared_gate, shared_up, shared_down)
    return (attended, moe_out)
```

```python
import numpy as np
import jax
import jax.numpy as jnp
from jax import lax
from jax.experimental import pallas as pl
from jax.experimental.pallas import tpu as pltpu
from jax.sharding import PartitionSpec as P

MESH = pl.DeviceIdType.MESH
BF = jnp.bfloat16
F32 = jnp.float32

HEAD_DIM = 128
WINDOW = 128
GRID_W = 64
D = 4096
TOP_K = 4
EPS = 1e-06
ROTARY_BASE = 10000.0

NZ = 16
TOK = 160
TPAD = 256
SLOT = 32
ROWS = 32 * SLOT
LEN = 512
FEAT = 256
UNITS = 128
PACK = 64

REL = [0, 1, -1, 8, 7, -7, 6, -6, 5, -5, 4, -4, 3, -3, 2, -2]


def _inv(p):
    return REL.index(REL[p] if REL[p] in (0, 8) else -REL[p])


INV = [_inv(p) for p in range(NZ)]
CHUNK = 256
NCHUNK = ROWS // CHUNK

GATHER_1 = [(c * CHUNK, CHUNK) for c in range(NCHUNK)] + [(ROWS, TOK)]
GATHER_2 = [(c * CHUNK, CHUNK) for c in range(NCHUNK)] + [(ROWS, PACK)]
OWN = NCHUNK


def up16(v):
    return (v + 15) // 16 * 16


def kernel(
    x_ref,
    ids_ref,
    rw_ref,
    q_ref,
    k_ref,
    v_ref,
    qg_ref,
    kg_ref,
    sink_ref,
    ng_ref,
    colt_ref,
    rowt_hbm,
    gate_hbm,
    up_hbm,
    down_hbm,
    sg_ref,
    su_ref,
    sd_hbm,
    att_ref,
    out_ref,
    xg,
    hg,
    wgu,
    wd,
    wsd,
    rowt,
    kpad,
    vpad,
    qt,
    kt,
    xpad,
    idsp,
    rwp,
    send,
    wt_hi,
    wt_lo,
    lhs,
    res,
    ret,
    acc,
    sh_acc,
    bar_dummy,
    g_send,
    g_recv,
    zi_send,
    zi_recv,
    zo_send,
    zo_recv,
    halo_send,
    halo_recv,
    loc,
):
    ep = lax.axis_index("ep")
    tp = lax.axis_index("tp")
    z = ep // 2
    core = ep % 2
    y = tp // 4
    x = tp % 4
    xr, xl = (x + 1) % 4, (x + 3) % 4
    yr, yl = (y + 1) % 4, (y + 3) % 4

    def ep_at(rel, c):
        return ((z + rel + NZ) % NZ) * 2 + c

    ep_hi = (ep + 1) % 32
    ep_lo = (ep + 31) % 32

    barrier = pltpu.get_barrier_semaphore()
    for p in range(NZ):
        for c in range(2):
            if p == 0:
                continue
            pl.semaphore_signal(
                barrier, inc=1, device_id={"ep": ep_at(REL[p], c), "tp": tp}, device_id_type=MESH
            )
    pl.semaphore_signal(
        barrier, inc=1, device_id={"ep": z * 2 + (1 - core), "tp": tp}, device_id_type=MESH
    )
    plane = [y * 4 + xr, y * 4 + xl, yr * 4 + x, yl * 4 + x]
    for t in plane:
        pl.semaphore_signal(barrier, inc=1, device_id={"ep": ep, "tp": t}, device_id_type=MESH)

    loads = [
        pltpu.make_async_copy(gate_hbm.at[0], wgu.at[:, 0:128], loc.at[0]),
        pltpu.make_async_copy(up_hbm.at[0], wgu.at[:, 128:256], loc.at[1]),
        pltpu.make_async_copy(down_hbm.at[0], wd, loc.at[2]),
        pltpu.make_async_copy(
            rowt_hbm.at[:, pl.ds(pl.multiple_of(ep * 8, 8), 16), :], rowt, loc.at[3]
        ),
    ] + [
        pltpu.make_async_copy(sd_hbm, wsd.at[:, pl.ds(32 * j, 32), :], loc.at[4 + j])
        for j in range(4)
    ]
    for cp in loads:
        cp.start()

    xg[y, x, ROWS : ROWS + TOK, :] = x_ref[...]
    xpad[...] = jnp.zeros_like(xpad)
    xpad[0:TOK, :] = x_ref[...]
    idsp[...] = jnp.full(idsp.shape, -1, jnp.int32)
    idsp[0:TOP_K, 0:TOK] = ids_ref[...]
    rwp[...] = jnp.zeros_like(rwp)
    rwp[0:TOP_K, 0:TOK] = rw_ref[...]
    kpad[WINDOW : WINDOW + LEN, :] = k_ref[...]
    vpad[WINDOW : WINDOW + LEN, :] = v_ref[...]

    row32 = lax.broadcasted_iota(jnp.int32, (32, TPAD), 0)
    pos32 = row32 >> 1
    rel32 = jnp.zeros((32, TPAD), jnp.int32)
    for p in range(NZ):
        rel32 = jnp.where(pos32 == p, REL[p] + NZ, rel32)
    expert32 = ((z + rel32) & (NZ - 1)) * 2 + (row32 & 1)
    named = jnp.zeros((32, TPAD), F32)
    weight = jnp.zeros((32, TPAD), F32)
    for k in range(TOP_K):
        same = idsp[k : k + 1, :] == expert32
        named = jnp.where(same, 1.0, named)
        weight = jnp.where(same, rwp[k : k + 1, :], weight)
    before = (
        lax.broadcasted_iota(jnp.int32, (TPAD, TPAD), 0)
        < lax.broadcasted_iota(jnp.int32, (TPAD, TPAD), 1)
    )
    count = jnp.dot(
        named.astype(BF), jnp.where(before, 1.0, 0.0).astype(BF), preferred_element_type=F32
    )
    slot32 = jnp.where(named > 0.5, count, -1.0)
    slot_row = lax.broadcasted_iota(jnp.int32, (SLOT, TPAD), 0).astype(F32)
    for t in range(NCHUNK):
        picks = [
            jnp.where(slot32[i : i + 1, :] == slot_row, 1.0, 0.0).astype(BF)
            for i in range(8 * t, 8 * t + 8)
        ]
        send[CHUNK * t : CHUNK * (t + 1), :] = jnp.dot(
            jnp.concatenate(picks, axis=0), xpad[...], preferred_element_type=F32
        ).astype(BF)
    xg[y, x, pl.ds(pl.multiple_of(core * SLOT, SLOT), SLOT), :] = send[
        pl.ds(pl.multiple_of(core * SLOT, SLOT), SLOT), :
    ]

    pl.semaphore_wait(barrier, 35)

    sends = []

    def remote(src, dst, ssem, rsem, dev):
        cp = pltpu.make_async_remote_copy(
            src_ref=src,
            dst_ref=dst,
            send_sem=ssem,
            recv_sem=rsem,
            device_id=dev,
            device_id_type=MESH,
        )
        sends.append(cp)
        return cp

    class Gather:
        def __init__(self, which, buf, start, size, index):
            self.buf, self.index, self.which = buf, index, which
            na = up16(size // 2)
            self.ranges = []
            for first, count in ((start, na), (start + na, size - na)):
                low = up16(count // 2)
                self.ranges.append((first, count, low))
            self.stage = 0
            self.pending = []

        def next(self):
            for cp in self.pending:
                cp.wait_recv()
            self.pending = []
            s = self.stage
            self.stage += 1
            if s == 4:
                return
            buf = self.buf
            for half, (first, count, low) in enumerate(self.ranges):
                full = pl.ds(first, count)
                part_lo, part_hi = pl.ds(first, low), pl.ds(first + low, count - low)
                if half == 0:
                    near = lambda v, r: buf.at[y, v, r]
                    wide = lambda v, r: buf.at[v, :, r]
                    n_me, n_r, n_l, w_me, w_r, w_l = x, xr, xl, y, yr, yl
                    to_nr, to_nl = y * 4 + xr, y * 4 + xl
                    to_wr, to_wl = yr * 4 + x, yl * 4 + x
                else:
                    near = lambda v, r: buf.at[v, x, r]
                    wide = lambda v, r: buf.at[:, v, r]
                    n_me, n_r, n_l, w_me, w_r, w_l = y, yr, yl, x, xr, xl
                    to_nr, to_nl = yr * 4 + x, yl * 4 + x
                    to_wr, to_wl = y * 4 + xr, y * 4 + xl
                if s == 0:
                    pair = ((near(n_me, full), to_nr), (near(n_me, full), to_nl))
                elif s == 1:
                    pair = ((near(n_l, part_lo), to_nr), (near(n_r, part_hi), to_nl))
                elif s == 2:
                    pair = ((wide(w_me, full), to_wr), (wide(w_me, full), to_wl))
                else:
                    pair = ((wide(w_l, part_lo), to_wr), (wide(w_r, part_hi), to_wl))
                for direction, (ref, to) in enumerate(pair):
                    i = ((self.which * 5 + self.index) * 2 + half) * 8 + s * 2 + direction
                    cp = remote(ref, ref, g_send.at[i], g_recv.at[i], {"ep": ep, "tp": to})
                    cp.start()
                    self.pending.append(cp)

    rows_g = [Gather(0, xg, s, n, i) for i, (s, n) in enumerate(GATHER_1)]
    hid_g = [Gather(1, hg, s, n, i) for i, (s, n) in enumerate(GATHER_2)]

    zin = {}

    def start_zin(p):
        for c in range(2):
            if p == 0:
                if c == 1:
                    continue
                c = 1 - core
            src = send.at[pl.ds(pl.multiple_of(p * 2 * SLOT + c * SLOT, SLOT), SLOT)]
            q = INV[p]
            dst = xg.at[y, x, pl.ds(pl.multiple_of(q * 2 * SLOT + core * SLOT, SLOT), SLOT)]
            cp = remote(
                src,
                dst,
                zi_send.at[2 * p + c],
                zi_recv.at[2 * q + core],
                {"ep": ep_at(REL[p], c), "tp": tp},
            )
            cp.start()

    def wait_block(buf_at, recv, p):
        for c in range(2):
            if p == 0:
                if c == 1:
                    continue
                c = 1 - core
            dst = buf_at(pl.ds(pl.multiple_of(p * 2 * SLOT + c * SLOT, SLOT), SLOT))
            pltpu.make_async_remote_copy(
                src_ref=dst,
                dst_ref=dst,
                send_sem=zi_send.at[0],
                recv_sem=recv.at[2 * p + c],
                device_id={"ep": z * 2 + (1 - core), "tp": tp},
                device_id_type=MESH,
            ).wait_recv()

    def wait_zin(chunk):
        for p in range(4 * chunk, 4 * chunk + 4):
            wait_block(lambda r: xg.at[y, x, r], zi_recv, p)

    def start_zout(chunk):
        for p in range(4 * chunk, 4 * chunk + 4):
            q = INV[p]
            for c in range(2):
                if p == 0:
                    if c == 1:
                        continue
                    c = 1 - core
                src = res.at[pl.ds(pl.multiple_of(p * 2 * SLOT + c * SLOT, SLOT), SLOT)]
                dst = ret.at[pl.ds(pl.multiple_of(q * 2 * SLOT + core * SLOT, SLOT), SLOT)]
                cp = remote(
                    src,
                    dst,
                    zo_send.at[2 * p + c],
                    zo_recv.at[2 * q + core],
                    {"ep": ep_at(REL[p], c), "tp": tp},
                )
                cp.start()

    def wait_zout(chunk):
        for p in range(4 * chunk, 4 * chunk + 4):
            wait_block(lambda r: ret.at[r], zo_recv, p)

    halos = []

    def start_halo():
        tail, head = pl.ds(LEN - WINDOW, WINDOW), pl.ds(0, WINDOW)
        for i, (ref, pad) in enumerate(((k_ref, kpad), (v_ref, vpad))):
            for j, (part, to, at) in enumerate(
                ((tail, ep_hi, head), (head, ep_lo, pl.ds(WINDOW + LEN, WINDOW)))
            ):
                cp = remote(
                    ref.at[part],
                    pad.at[at],
                    halo_send.at[2 * i + j],
                    halo_recv.at[2 * i + j],
                    {"ep": to, "tp": tp},
                )
                cp.start()
                halos.append(cp)

    first_half = (lax.broadcasted_iota(jnp.int32, (GRID_W, HEAD_DIM), 1) & 63) < 32

    def turn(raw, gain, g):
        f = raw.astype(F32)
        n = f * lax.rsqrt(jnp.mean(f * f, axis=-1, keepdims=True) + EPS) * gain
        other = jnp.where(first_half, pltpu.roll(n, 96, 1), pltpu.roll(n, 32, 1))
        cos = rowt[0, pl.ds(g, 1), :] + colt_ref[0]
        sin = rowt[1, pl.ds(g, 1), :] + colt_ref[1]
        return (n * cos + other * sin).astype(BF)

    def turn_queries():
        for g in range(LEN // GRID_W):
            for h in range(2):
                rows = slice(g * GRID_W, (g + 1) * GRID_W)
                qt[h, rows, :] = turn(
                    q_ref[rows, h * HEAD_DIM : (h + 1) * HEAD_DIM], qg_ref[...], g + 2
                )

    def turn_keys():
        for g in range((LEN + 2 * WINDOW) // GRID_W):
            rows = slice(g * GRID_W, (g + 1) * GRID_W)
            kt[rows, :] = turn(kpad[rows, :], kg_ref[...], g)

    near_q = lax.broadcasted_iota(jnp.int32, (128, 384), 0)
    near_k = lax.broadcasted_iota(jnp.int32, (128, 384), 1)

    def attend(b):
        key_pos = near_k + (ep * LEN - WINDOW + 128 * b)
        inside = (
            (near_k >= near_q)
            & (near_k <= near_q + 2 * WINDOW)
            & (key_pos >= 0)
            & (key_pos < 32 * LEN)
        )
        keys = kt[128 * b : 128 * b + 384, :]
        values = vpad[128 * b : 128 * b + 384, :]
        for h in range(2):
            scores = lax.dot_general(
                qt[h, 128 * b : 128 * b + 128, :],
                keys,
                (((1,), (1,)), ((), ())),
                preferred_element_type=F32,
            ) * (HEAD_DIM ** (-0.5))
            raised = jnp.where(inside, jnp.exp(scores), 0.0)
            sink = jnp.exp(jnp.full((128, 1), sink_ref[h], F32))
            den = sink + jnp.sum(raised, axis=-1, keepdims=True)
            weights = (raised * (1.0 / den)).astype(BF)
            mixed = jnp.dot(weights, values, preferred_element_type=F32)
            att_ref[128 * b : 128 * b + 128, h * 128 : (h + 1) * 128] = mixed.astype(BF)

    def scale_rows(start, size):
        acc[0:size, 0:128] = jnp.zeros((size, 128), F32)

        def one(s, carry):
            f = xg[s // 4, s % 4, start : start + size, :].astype(F32)
            sq = f * f
            acc[0:size, 0:128] += sq[:, 0:128] + sq[:, 128:256]
            lhs[s, 0:size, :] = (f * ng_ref[pl.ds(s, 1), :]).astype(BF)
            return carry

        lax.fori_loop(0, 16, one, 0)
        return lax.rsqrt(jnp.sum(acc[0:size, 0:128], axis=-1, keepdims=True) / D + EPS)

    def activate(g, u, factor):
        g, u = g * factor, u * factor
        return (g / (1.0 + jnp.exp(-g)) * u).astype(BF)

    def experts_in(c):
        start = c * CHUNK
        factor = scale_rows(start, CHUNK)
        both = jnp.dot(
            jnp.concatenate([lhs[s] for s in range(16)], axis=1),
            wgu[...],
            preferred_element_type=F32,
        )
        hg[y, x, start : start + CHUNK, :] = activate(both[:, 0:128], both[:, 128:256], factor)

    def shared_in():
        factor = scale_rows(ROWS, TOK)
        rows = jnp.concatenate([lhs[s, 0:TOK, :] for s in range(16)], axis=1)
        g = jnp.dot(rows, sg_ref[...], preferred_element_type=F32)
        u = jnp.dot(rows, su_ref[...], preferred_element_type=F32)
        h = activate(g, u, factor).astype(F32)
        packed = jnp.concatenate([h[40 * j : 40 * j + 40, :] for j in range(4)], axis=1)
        packed = jnp.concatenate([packed, jnp.zeros((PACK - 40, 128), F32)], axis=0)
        hg[y, x, ROWS : ROWS + PACK, :] = packed.astype(BF)

    def experts_out(c):
        start = c * CHUNK
        rows = jnp.concatenate(
            [hg[s // 4, s % 4, start : start + CHUNK, :] for s in range(16)], axis=1
        )
        res[start : start + CHUNK, :] = jnp.dot(
            rows, wd[...], preferred_element_type=F32
        ).astype(BF)
        if c == 0:
            mine = pl.ds(pl.multiple_of(core * SLOT, SLOT), SLOT)
            ret[mine, :] = res[mine, :]

    def shared_out():
        group = lax.broadcasted_iota(jnp.int32, (40, 128), 1) // 32
        total = jnp.zeros((TOK, FEAT), F32)
        for s in range(16):
            piece = hg[s // 4, s % 4, ROWS : ROWS + PACK, :].astype(F32)[0:40, :]
            parts = jnp.concatenate(
                [jnp.where(group == j, piece, 0.0) for j in range(4)], axis=0
            )
            total += jnp.dot(parts.astype(BF), wsd[s], preferred_element_type=F32)
        sh_acc[...] = total

    def combine_weights():
        for t in range(NCHUNK):
            full = jnp.concatenate(
                [
                    jnp.where(slot32[i : i + 1, :] == slot_row, weight[i : i + 1, :], 0.0)
                    for i in range(8 * t, 8 * t + 8)
                ],
                axis=0,
            )
            turned = jnp.transpose(full)
            high = turned.astype(BF)
            wt_hi[t] = high
            wt_lo[t] = (turned - high.astype(F32)).astype(BF)

    def combine(c):
        rows = ret[c * CHUNK : (c + 1) * CHUNK, :]
        part = jnp.dot(wt_hi[c], rows, preferred_element_type=F32) + jnp.dot(
            wt_lo[c], rows, preferred_element_type=F32
        )
        sh_acc[...] += part[0:TOK, :]

    R1, R2, R3, R4, O1 = rows_g
    H1, H2, H3, H4, S2 = hid_g

    O1.next()
    for p in range(NZ):
        start_zin(p)
    start_halo()
    combine_weights()
    for cp in loads[3:]:
        cp.wait()
    O1.next()
    wait_zin(0)
    R1.next()
    O1.next()
    turn_queries()
    R1.next()
    O1.next()
    wait_zin(1)
    R2.next()
    R1.next()
    for cp in halos:
        cp.wait_recv()
    turn_keys()
    O1.next()
    R2.next()
    shared_in()
    S2.next()
    R1.next()
    attend(0)
    S2.next()
    wait_zin(2)
    R3.next()
    R2.next()
    attend(1)
    S2.next()
    R1.next()
    for cp in loads[:3]:
        cp.wait()
    experts_in(0)
    H1.next()
    R3.next()
    R2.next()
    S2.next()
    H1.next()
    wait_zin(3)
    R4.next()
    R3.next()
    attend(2)
    R2.next()
    experts_in(1)
    H2.next()
    H1.next()
    R4.next()
    R3.next()
    H2.next()
    S2.next()
    shared_out()
    R4.next()
    attend(3)
    R3.next()
    experts_in(2)
    H3.next()
    H1.next()
    H2.next()
    R4.next()
    H3.next()
    H1.next()
    experts_out(0)
    start_zout(0)
    H2.next()
    H3.next()
    R4.next()
    experts_in(3)
    H4.next()
    H2.next()
    experts_out(1)
    start_zout(1)
    H3.next()
    H4.next()
    wait_zout(0)
    combine(0)
    H4.next()
    H3.next()
    experts_out(2)
    start_zout(2)
    H4.next()
    wait_zout(1)
    combine(1)
    H4.next()
    experts_out(3)
    start_zout(3)
    wait_zout(2)
    combine(2)
    wait_zout(3)
    combine(3)
    out_ref[...] = sh_acc[...].astype(BF)
    for cp in sends:
        cp.wait_send()


def _tables():
    quarter = HEAD_DIM // 4
    freq = np.float32(ROTARY_BASE) ** (
        np.float32(-4.0) * np.arange(quarter, dtype=np.float32) / np.float32(HEAD_DIM)
    )
    freq = freq.astype(np.float32)
    sign = np.concatenate([-np.ones(quarter), np.ones(quarter)])

    def of(index):
        angle = (index.astype(np.float32)[:, None] * freq).astype(np.float32).astype(np.float64)
        angle = np.concatenate([angle, angle], axis=1)
        return np.cos(angle), np.sin(angle) * sign

    def put(pair, left):
        pads = [(0, 0), (0, 64)] if left else [(0, 0), (64, 0)]
        return np.stack([np.pad(v, pads) for v in pair]).astype(np.float32)

    rows = put(of(np.arange(-2, 270)), True)
    cols = put(of(np.arange(GRID_W)), False)
    return rows, cols


ROW_TABLE, COL_TABLE = _tables()


def shards(
    query_vectors,
    key_vectors,
    value_vectors,
    query_gain,
    key_gain,
    sink_logits,
    moe_rows,
    norm_gain,
    expert_ids,
    route_weights,
    expert_gate,
    expert_up,
    expert_down,
    shared_gate,
    shared_up,
    shared_down,
):
    vm = pl.BlockSpec(memory_space=pltpu.VMEM)
    sm = pl.BlockSpec(memory_space=pltpu.SMEM)
    hb = pl.BlockSpec(memory_space=pl.ANY)
    dma = pltpu.SemaphoreType.DMA
    return pl.pallas_call(
        kernel,
        out_shape=(
            jax.ShapeDtypeStruct((LEN, 2 * HEAD_DIM), BF),
            jax.ShapeDtypeStruct((TOK, FEAT), BF),
        ),
        in_specs=[vm] * 8 + [sm] + [vm] * 2 + [hb] * 4 + [vm] * 2 + [hb],
        out_specs=(vm, vm),
        scratch_shapes=[
            pltpu.VMEM((4, 4, ROWS + TOK, FEAT), BF),
            pltpu.VMEM((4, 4, ROWS + PACK, UNITS), BF),
            pltpu.VMEM((D, 2 * UNITS), BF),
            pltpu.VMEM((16 * UNITS, FEAT), BF),
            pltpu.VMEM((16, 128, FEAT), BF),
            pltpu.VMEM((2, 16, 128), F32),
            pltpu.VMEM((LEN + 2 * WINDOW, HEAD_DIM), BF),
            pltpu.VMEM((LEN + 2 * WINDOW, HEAD_DIM), BF),
            pltpu.VMEM((2, LEN, HEAD_DIM), BF),
            pltpu.VMEM((LEN + 2 * WINDOW, HEAD_DIM), BF),
            pltpu.VMEM((TPAD, FEAT), BF),
            pltpu.VMEM((8, TPAD), jnp.int32),
            pltpu.VMEM((8, TPAD), F32),
            pltpu.VMEM((ROWS, FEAT), BF),
            pltpu.VMEM((NCHUNK, TPAD, CHUNK), BF),
            pltpu.VMEM((NCHUNK, TPAD, CHUNK), BF),
            pltpu.VMEM((16, CHUNK, FEAT), BF),
            pltpu.VMEM((ROWS, FEAT), BF),
            pltpu.VMEM((ROWS, FEAT), BF),
            pltpu.VMEM((CHUNK, 128), F32),
            pltpu.VMEM((TOK, FEAT), F32),
            pltpu.SMEM((1,), jnp.int32),
            dma((160,)),
            dma((160,)),
            dma((32,)),
            dma((32,)),
            dma((32,)),
            dma((32,)),
            dma((4,)),
            dma((4,)),
            dma((8,)),
        ],
        compiler_params=pltpu.CompilerParams(
            collective_id=0, has_side_effects=True, vmem_limit_bytes=50 * 1024 * 1024
        ),
        name="fused",
    )(
        moe_rows,
        expert_ids.T,
        route_weights.T,
        query_vectors,
        key_vectors,
        value_vectors,
        query_gain.reshape(1, HEAD_DIM),
        key_gain.reshape(1, HEAD_DIM),
        sink_logits,
        norm_gain.reshape(16, FEAT),
        jnp.asarray(COL_TABLE),
        jnp.asarray(ROW_TABLE),
        expert_gate,
        expert_up,
        expert_down,
        shared_gate,
        shared_up,
        shared_down.reshape(16, 32, FEAT),
    )


def solution(mesh):
    placed = (
        P("ep", "tp"),
        P("ep", "tp"),
        P("ep", "tp"),
        P(),
        P(),
        P("tp"),
        P("ep", "tp"),
        P(),
        P("ep", None),
        P("ep", None),
        P("ep", None, "tp"),
        P("ep", None, "tp"),
        P("ep", None, "tp"),
        P(None, "tp"),
        P(None, "tp"),
        P(None, "tp"),
    )
    return jax.shard_map(
        shards,
        mesh=mesh,
        in_specs=placed,
        out_specs=(P("ep", "tp"), P("ep", "tp")),
        check_vma=False,
    )
```

```python
import numpy as np
import jax
import jax.numpy as jnp
from jax import lax
from jax.experimental import pallas as pl
from jax.experimental.pallas import tpu as pltpu
from jax.sharding import PartitionSpec as P

MESH = pl.DeviceIdType.MESH
BF = jnp.bfloat16
F32 = jnp.float32

HEAD_DIM = 128
WINDOW = 128
GRID_W = 64
D = 4096
TOP_K = 4
EPS = 1e-06
ROTARY_BASE = 10000.0

NZ = 16
TOK = 160
TPAD = 256
SLOT = 32
ROWS = 32 * SLOT
LEN = 512
FEAT = 256
UNITS = 128
PACK = 40

GROUPS = [[1, -1], [6, -6], [7, -7], [8], [5, -5], [4, -4], [3, -3], [2, -2], [0]]
REL = sum(GROUPS, [])
NCHUNK = len(GROUPS)
ZFIRST = [2 * SLOT * sum(len(g) for g in GROUPS[:c]) for c in range(NCHUNK)]
ZSIZE = [2 * SLOT * len(g) for g in GROUPS]
SIZE = [(60 * len(g) + 7) // 8 * 8 for g in GROUPS]
FIRST = [sum(SIZE[:c]) for c in range(NCHUNK)]
PACKED = sum(SIZE)
HERE = REL.index(0)
OWN_CHUNK = [c for c in range(NCHUNK) if 0 in GROUPS[c]][0]


def _inv(p):
    return REL.index(REL[p] if REL[p] in (0, 8) else -REL[p])


INV = [_inv(p) for p in range(NZ)]
CHUNK = 256

GATHER_1 = list(zip(FIRST, SIZE)) + [(PACKED, TOK)]
GATHER_2 = list(zip(FIRST, SIZE)) + [(PACKED, PACK)]
NGATHER = NCHUNK + 1

ORDER = (
    "R9", "zi:0", "halo", "zi:1", "zi:2", "zi:3", "zi:4", "zi:5", "zi:6", "zi:7", "zi:8",
    "cw", "lda", "lds", "ldb", "tq", "wi:8", "R8", "wi:0", "R0", "wh", "tk", "R9", "at:0",
    "at:1", "at:2", "at:3", "R8", "R0", "R9", "R8", "R0", "wi:1", "R1", "R9", "R8", "R0",
    "R1", "R9", "si", "H9", "wi:2", "R2", "R8", "ei:8", "H8", "R1", "R0", "ei:0", "H0",
    "wi:3", "R3", "R2", "H9", "H8", "wi:4", "R4", "R1", "H0", "R3", "R2", "wi:5", "R5",
    "H9", "H8", "R4", "R1", "ei:1", "H1", "H0", "R3", "R2", "R5", "H9", "H8", "R4", "H1",
    "H0", "R3", "R2", "ei:2", "H2", "R5", "H9", "so", "wi:6", "R6", "H1", "R4", "H8",
    "eo:8", "zo:8", "wi:7", "R7", "H0", "eo:0", "zo:0", "H2", "R3", "ei:3", "H3", "R5",
    "R6", "H1", "wo:0", "cb:0-128", "R4", "ei:4", "H4", "H2", "R7", "H3", "R5", "ei:5",
    "H5", "R6", "H1", "eo:1", "zo:1", "H2", "H4", "R7", "H3", "H5", "R6", "H2", "eo:2",
    "zo:2", "H4", "R7", "H3", "H5", "R6", "ei:6", "H6", "H4", "R7", "ei:7", "H7", "H5",
    "H3", "eo:3", "zo:3", "H6", "wo:1", "cb:128-256", "H4", "eo:4", "zo:4", "H7", "H5",
    "eo:5", "zo:5", "H6", "H7", "wo:2", "cb:256-384", "H6", "H7", "H6", "eo:6", "zo:6",
    "H7", "eo:7", "zo:7", "wo:3", "wo:4", "cb:384-512", "wo:5", "cb:512-640", "wo:6",
    "cb:640-768", "wo:7", "cb:768-896", "wo:8", "cb:896-1024", "end",
)


def up8(v):
    return (v + 7) // 8 * 8


def kernel(
    x_hbm,
    ids_hbm,
    rw_hbm,
    q_hbm,
    k_hbm,
    v_hbm,
    qg_hbm,
    kg_hbm,
    sink_hbm,
    ng_hbm,
    colt_hbm,
    rowt_hbm,
    gate_hbm,
    up_hbm,
    down_hbm,
    sg_hbm,
    su_hbm,
    sd_hbm,
    att_ref,
    out_ref,
    ids_ref,
    rw_ref,
    q_ref,
    qg_ref,
    kg_ref,
    sink_ref,
    ng_ref,
    colt_ref,
    sg_ref,
    su_ref,
    xg,
    hg,
    wgu,
    wd,
    wsd,
    rowt,
    kpad,
    vpad,
    qt,
    kt,
    xpad,
    idsp,
    rwp,
    send,
    wt_hi,
    wt_lo,
    lhs,
    res,
    ret,
    acc,
    sh_acc,
    zst,
    pick,
    spread,
    g_send,
    g_recv,
    zi_send,
    zi_recv,
    zo_send,
    zo_recv,
    halo_sem,
    loc,
):
    ep = lax.axis_index("ep")
    tp = lax.axis_index("tp")
    z = ep // 2
    core = ep % 2
    y = tp // 4
    x = tp % 4
    xr, xl = (x + 1) % 4, (x + 3) % 4
    yr, yl = (y + 1) % 4, (y + 3) % 4
    xo, yo = (x + 2) % 4, (y + 2) % 4

    def ep_at(rel, c):
        return ((z + rel + NZ) % NZ) * 2 + c

    ep_hi = (ep + 1) % 32
    ep_lo = (ep + 31) % 32

    barrier = pltpu.get_barrier_semaphore()
    for p in range(NZ):
        for c in range(2):
            if REL[p] == 0:
                continue
            pl.semaphore_signal(
                barrier, inc=1, device_id={"ep": ep_at(REL[p], c), "tp": tp}, device_id_type=MESH
            )
    pl.semaphore_signal(
        barrier, inc=1, device_id={"ep": z * 2 + (1 - core), "tp": tp}, device_id_type=MESH
    )
    plane = [y * 4 + xr, y * 4 + xl, yr * 4 + x, yl * 4 + x]
    for t in plane:
        pl.semaphore_signal(barrier, inc=1, device_id={"ep": ep, "tp": t}, device_id_type=MESH)

    def load(i, src, dst):
        cp = pltpu.make_async_copy(src, dst, loc.at[i])
        cp.start()
        return cp

    mid = pl.ds(WINDOW, LEN)
    rows_at = pl.ds(PACKED, TOK)
    ld_own = load(0, x_hbm, xg.at[y, x, rows_at])
    ld_route = [
        load(1, ids_hbm, ids_ref),
        load(2, rw_hbm, rw_ref),
        load(3, x_hbm, xpad.at[pl.ds(0, TOK)]),
    ]
    ld_kv = [load(4, k_hbm, kpad.at[mid]), load(5, v_hbm, vpad.at[mid])]
    ld_att = [
        load(6, q_hbm, q_ref),
        load(7, qg_hbm, qg_ref),
        load(8, kg_hbm, kg_ref),
        load(9, sink_hbm, sink_ref),
        load(10, colt_hbm, colt_ref),
        load(11, rowt_hbm.at[:, pl.ds(pl.multiple_of(ep * 8, 8), 16), :], rowt),
    ]
    ld_shared = [load(12, sg_hbm, sg_ref), load(13, su_hbm, su_ref), load(14, ng_hbm, ng_ref)] + [
        load(15 + j, sd_hbm, wsd.at[:, pl.ds(32 * j, 32), :]) for j in range(4)
    ]
    ld_big = [
        load(19, gate_hbm.at[0], wgu.at[:, 0:128]),
        load(20, up_hbm.at[0], wgu.at[:, 128:256]),
        load(21, down_hbm.at[0], wd),
    ]

    def wait_all(copies):
        for cp in copies:
            cp.wait()

    xpad[TOK:TPAD, :] = jnp.zeros((TPAD - TOK, FEAT), BF)
    idsp[...] = jnp.full(idsp.shape, -1, jnp.int32)
    rwp[...] = jnp.zeros_like(rwp)
    wait_all(ld_route)
    idsp[0:TOP_K, 0:TOK] = ids_ref[...]
    rwp[0:TOP_K, 0:TOK] = rw_ref[...]

    row32 = lax.broadcasted_iota(jnp.int32, (32, TPAD), 0)
    pos32 = row32 >> 1
    rel32 = jnp.zeros((32, TPAD), jnp.int32)
    for p in range(NZ):
        rel32 = jnp.where(pos32 == p, REL[p] + NZ, rel32)
    expert32 = ((z + rel32) & (NZ - 1)) * 2 + (row32 & 1)
    named = jnp.zeros((32, TPAD), F32)
    weight = jnp.zeros((32, TPAD), F32)
    for k in range(TOP_K):
        same = idsp[k : k + 1, :] == expert32
        named = jnp.where(same, 1.0, named)
        weight = jnp.where(same, rwp[k : k + 1, :], weight)
    before = (
        lax.broadcasted_iota(jnp.int32, (TPAD, TPAD), 0)
        < lax.broadcasted_iota(jnp.int32, (TPAD, TPAD), 1)
    )
    count = jnp.dot(
        named.astype(BF), jnp.where(before, 1.0, 0.0).astype(BF), preferred_element_type=F32
    )
    slot32 = jnp.where(named > 0.5, count, -1.0)
    slot_row = lax.broadcasted_iota(jnp.int32, (SLOT, TPAD), 0).astype(F32)
    for t in range(NCHUNK):
        lo, n = ZFIRST[t], ZSIZE[t]
        picks = [
            jnp.where(slot32[i : i + 1, :] == slot_row, 1.0, 0.0).astype(BF)
            for i in range(lo // SLOT, (lo + n) // SLOT)
        ]
        send[lo : lo + n, :] = jnp.dot(
            jnp.concatenate(picks, axis=0), xpad[...], preferred_element_type=F32
        ).astype(BF)
    mine = pl.ds(pl.multiple_of(HERE * 2 * SLOT + core * SLOT, SLOT), SLOT)
    other = pl.ds(pl.multiple_of(HERE * 2 * SLOT + (1 - core) * SLOT, SLOT), SLOT)
    zst[mine, :] = send[mine, :]

    def moved(r):
        over = [jnp.where(r >= 30 * i, 2, 0) for i in (1, 2, 3)]
        return r + over[0] + over[1] + over[2]

    iota = lambda shape, axis: lax.broadcasted_iota(jnp.int32, shape, axis)
    wide_shape, tall_shape = (120, 128), (128, 120)
    pick[...] = jnp.where(
        moved(iota(wide_shape, 0)) == iota(wide_shape, 1), 1.0, 0.0
    ).astype(BF)
    spread[...] = jnp.where(
        iota(tall_shape, 0) == moved(iota(tall_shape, 1)), 1.0, 0.0
    ).astype(BF)

    def pack(c):
        rows = jnp.dot(
            pick[0 : SIZE[c], 0 : ZSIZE[c]],
            zst[ZFIRST[c] : ZFIRST[c] + ZSIZE[c], :],
            preferred_element_type=F32,
        )
        xg[y, x, FIRST[c] : FIRST[c] + SIZE[c], :] = rows.astype(BF)

    ld_own.wait()
    pl.semaphore_wait(barrier, 35)

    ends = []

    def remote(src, dst, ssem, rsem, dev):
        cp = pltpu.make_async_remote_copy(
            src_ref=src,
            dst_ref=dst,
            send_sem=ssem,
            recv_sem=rsem,
            device_id=dev,
            device_id_type=MESH,
        )
        return cp

    partner = {"ep": z * 2 + (1 - core), "tp": tp}

    class Gather:
        def __init__(self, which, buf, start, size, index):
            self.buf, self.width = buf, buf.shape[3]
            self.start, self.size = start, size
            self.index = which * NGATHER + index
            na = up8(size // 2)
            self.ranges = []
            for first, count in ((start, na), (start + na, size - na)):
                self.ranges.append((first, count, up8(count // 2)))
            self.stage = 0

        def next(self):
            s = self.stage
            self.stage += 1
            buf = self.buf
            ssem = g_send.at[self.index]
            if s > 0:
                rows = pl.ds(self.start, self.size)
                whole = (
                    buf.at[pl.ds(0, 2), 0, rows],
                    buf.at[0, 0, rows],
                    buf.at[pl.ds(0, 2), :, rows],
                    buf.at[0, :, rows],
                )[s - 1]
                rsem = g_recv.at[self.index * 4 + s - 1]
                remote(whole, whole, ssem, rsem, partner).wait_recv()
            if s == 4:
                whole = lhs.at[pl.ds(0, 15), pl.ds(0, self.size), pl.ds(0, self.width)]
                ends.append(remote(whole, whole, ssem, g_recv.at[self.index * 4], partner))
                return
            near, wide = [], []
            for half, (first, count, low) in enumerate(self.ranges):
                full = pl.ds(first, count)
                part_lo, part_hi = pl.ds(first, low), pl.ds(first + low, count - low)
                if half == 0:
                    piece = lambda w, v, r: buf.at[w, v, r]
                    group = lambda w, r: buf.at[w, :, r]
                    n_me, n_r, n_l, n_o, w_me, w_r, w_l = x, xr, xl, xo, y, yr, yl
                    to_n, to_w = (y * 4 + xr, y * 4 + xl), (yr * 4 + x, yl * 4 + x)
                else:
                    piece = lambda w, v, r: buf.at[v, w, r]
                    group = lambda w, r: buf.at[:, w, r]
                    n_me, n_r, n_l, n_o, w_me, w_r, w_l = y, yr, yl, yo, x, xr, xl
                    to_n, to_w = (yr * 4 + x, yl * 4 + x), (y * 4 + xr, y * 4 + xl)
                if s == 0:
                    near += [(piece(w_me, n_me, full), to, 0) for to in to_n]
                    wide += [(piece(w_me, n_me, full), to, 2) for to in to_w]
                elif s == 1:
                    near += [
                        (piece(w_me, n_l, part_lo), to_n[0], 1),
                        (piece(w_me, n_r, part_hi), to_n[1], 1),
                    ]
                    wide += [(piece(w_me, v, full), to, 2) for v in (n_l, n_r) for to in to_w]
                elif s == 2:
                    wide += [(piece(w_me, n_o, full), to, 2) for to in to_w]
                else:
                    wide += [
                        (group(w_l, part_lo), to_w[0], 3),
                        (group(w_r, part_hi), to_w[1], 3),
                    ]
            for ref, to, kind in near + wide:
                remote(
                    ref, ref, ssem, g_recv.at[self.index * 4 + kind], {"ep": ep, "tp": to}
                ).start()

    rows_g = [Gather(0, xg, s, n, i) for i, (s, n) in enumerate(GATHER_1)]
    hid_g = [Gather(1, hg, s, n, i) for i, (s, n) in enumerate(GATHER_2)]

    def z_start(chunk, src_at, dst_at, ssem, rsem):
        for p in range(ZFIRST[chunk] // (2 * SLOT), (ZFIRST[chunk] + ZSIZE[chunk]) // (2 * SLOT)):
            q = INV[p]
            back = pl.ds(pl.multiple_of(q * 2 * SLOT + core * SLOT, SLOT), SLOT)
            if REL[p] == 0:
                pieces = [(other, partner)]
            else:
                pieces = [
                    (
                        pl.ds(p * 2 * SLOT + c * SLOT, SLOT),
                        {"ep": ep_at(REL[p], c), "tp": tp},
                    )
                    for c in range(2)
                ]
            for rows, dev in pieces:
                remote(src_at(rows), dst_at(back), ssem.at[chunk], rsem.at[chunk], dev).start()
        rows = other if chunk == OWN_CHUNK else pl.ds(ZFIRST[chunk], ZSIZE[chunk])
        ends.append(remote(src_at(rows), src_at(rows), ssem.at[chunk], rsem.at[chunk], partner))

    def z_wait(chunk, at, rsem, ssem):
        rows = other if chunk == OWN_CHUNK else pl.ds(ZFIRST[chunk], ZSIZE[chunk])
        remote(at(rows), at(rows), ssem.at[chunk], rsem.at[chunk], partner).wait_recv()

    own_at = lambda r: zst.at[r]
    send_at = lambda r: send.at[r]
    res_at = lambda r: res.at[r]
    ret_at = lambda r: ret.at[r]

    def start_zin(chunk):
        z_start(chunk, send_at, own_at, zi_send, zi_recv)

    def wait_zin(chunk):
        z_wait(chunk, own_at, zi_recv, zi_send)
        pack(chunk)

    def start_zout(chunk):
        z_start(chunk, res_at, ret_at, zo_send, zo_recv)

    def wait_zout(chunk):
        z_wait(chunk, ret_at, zo_recv, zo_send)

    def start_halo():
        tail, head = pl.ds(LEN, WINDOW), pl.ds(WINDOW, WINDOW)
        wait_all(ld_kv)
        for i, pad in enumerate((kpad, vpad)):
            for j, (part, to, at) in enumerate(
                ((tail, ep_hi, pl.ds(0, WINDOW)), (head, ep_lo, pl.ds(WINDOW + LEN, WINDOW)))
            ):
                cp = remote(
                    pad.at[part],
                    pad.at[at],
                    halo_sem.at[0],
                    halo_sem.at[1],
                    {"ep": to, "tp": tp},
                )
                cp.start()
        ends.append(halo_all())

    def halo_all():
        ref = kpad.at[pl.ds(0, 4 * WINDOW)]
        return remote(ref, ref, halo_sem.at[0], halo_sem.at[1], partner)

    first_half = (lax.broadcasted_iota(jnp.int32, (GRID_W, HEAD_DIM), 1) & 63) < 32

    def turn(raw, gain, g):
        f = raw.astype(F32)
        n = f * lax.rsqrt(jnp.mean(f * f, axis=-1, keepdims=True) + EPS) * gain
        other = jnp.where(first_half, pltpu.roll(n, 96, 1), pltpu.roll(n, 32, 1))
        cos = rowt[0, pl.ds(g, 1), :] + colt_ref[0]
        sin = rowt[1, pl.ds(g, 1), :] + colt_ref[1]
        return (n * cos + other * sin).astype(BF)

    def turn_queries():
        for g in range(LEN // GRID_W):
            for h in range(2):
                rows = slice(g * GRID_W, (g + 1) * GRID_W)
                qt[h, rows, :] = turn(
                    q_ref[rows, h * HEAD_DIM : (h + 1) * HEAD_DIM], qg_ref[...], g + 2
                )

    def turn_keys():
        for g in range((LEN + 2 * WINDOW) // GRID_W):
            rows = slice(g * GRID_W, (g + 1) * GRID_W)
            kt[rows, :] = turn(kpad[rows, :], kg_ref[...], g)

    near_q = lax.broadcasted_iota(jnp.int32, (128, 384), 0)
    near_k = lax.broadcasted_iota(jnp.int32, (128, 384), 1)

    def attend(b):
        key_pos = near_k + (ep * LEN - WINDOW + 128 * b)
        inside = (
            (near_k >= near_q)
            & (near_k <= near_q + 2 * WINDOW)
            & (key_pos >= 0)
            & (key_pos < 32 * LEN)
        )
        keys = kt[128 * b : 128 * b + 384, :]
        values = vpad[128 * b : 128 * b + 384, :]
        for h in range(2):
            scores = lax.dot_general(
                qt[h, 128 * b : 128 * b + 128, :],
                keys,
                (((1,), (1,)), ((), ())),
                preferred_element_type=F32,
            ) * (HEAD_DIM ** (-0.5))
            raised = jnp.where(inside, jnp.exp(scores), 0.0)
            sink = jnp.exp(jnp.full((128, 1), sink_ref[h], F32))
            den = sink + jnp.sum(raised, axis=-1, keepdims=True)
            weights = (raised * (1.0 / den)).astype(BF)
            mixed = jnp.dot(weights, values, preferred_element_type=F32)
            att_ref[128 * b : 128 * b + 128, h * 128 : (h + 1) * 128] = mixed.astype(BF)

    def scale_rows(start, size):
        acc[0:size, 0:128] = jnp.zeros((size, 128), F32)

        def one(s, carry):
            f = xg[s // 4, s % 4, start : start + size, :].astype(F32)
            sq = f * f
            acc[0:size, 0:128] += sq[:, 0:128] + sq[:, 128:256]
            lhs[s, 0:size, :] = (f * ng_ref[:, pl.ds(pl.multiple_of(s * FEAT, FEAT), FEAT)]).astype(BF)
            return carry

        lax.fori_loop(0, 16, one, 0)
        return lax.rsqrt(jnp.sum(acc[0:size, 0:128], axis=-1, keepdims=True) / D + EPS)

    def activate(g, u, factor):
        g, u = g * factor, u * factor
        return (g / (1.0 + jnp.exp(-g)) * u).astype(BF)

    def experts_in(c):
        start, size = FIRST[c], SIZE[c]
        factor = scale_rows(start, size)
        both = jnp.dot(
            jnp.concatenate([lhs[s, 0:size, :] for s in range(16)], axis=1),
            wgu[...],
            preferred_element_type=F32,
        )
        hg[y, x, start : start + size, :] = activate(both[:, 0:128], both[:, 128:256], factor)

    def shared_in():
        factor = scale_rows(PACKED, TOK)
        rows = jnp.concatenate([lhs[s, 0:TOK, :] for s in range(16)], axis=1)
        across = (((1,), (1,)), ((), ()))
        g = lax.dot_general(rows, sg_ref[...], across, preferred_element_type=F32)
        u = lax.dot_general(rows, su_ref[...], across, preferred_element_type=F32)
        h = activate(g, u, factor).astype(F32)
        packed = jnp.concatenate([h[40 * j : 40 * j + 40, :] for j in range(4)], axis=1)
        hg[y, x, PACKED : PACKED + PACK, :] = packed.astype(BF)

    def experts_out(c):
        start, size = FIRST[c], SIZE[c]
        rows = jnp.concatenate(
            [hg[s // 4, s % 4, start : start + size, :] for s in range(16)], axis=1
        )
        packed = jnp.dot(rows, wd[...], preferred_element_type=F32).astype(BF)
        res[ZFIRST[c] : ZFIRST[c] + ZSIZE[c], :] = jnp.dot(
            spread[0 : ZSIZE[c], 0:size], packed, preferred_element_type=F32
        ).astype(BF)
        if c == OWN_CHUNK:
            ret[mine, :] = res[mine, :]

    def shared_out():
        group = lax.broadcasted_iota(jnp.int32, (40, 128), 1) // 32
        total = jnp.zeros((TOK, FEAT), F32)
        for s in range(16):
            piece = hg[s // 4, s % 4, PACKED : PACKED + PACK, :].astype(F32)[0:40, :]
            parts = jnp.concatenate(
                [jnp.where(group == j, piece, 0.0) for j in range(4)], axis=0
            )
            total += jnp.dot(parts.astype(BF), wsd[s], preferred_element_type=F32)
        sh_acc[...] = total

    def combine_weights():
        for t in range(ROWS // CHUNK):
            full = jnp.concatenate(
                [
                    jnp.where(slot32[i : i + 1, :] == slot_row, weight[i : i + 1, :], 0.0)
                    for i in range(8 * t, 8 * t + 8)
                ],
                axis=0,
            )
            turned = jnp.transpose(full)
            high = turned.astype(BF)
            rows = slice(t * CHUNK, (t + 1) * CHUNK)
            wt_hi[:, rows] = high
            wt_lo[:, rows] = (turned - high.astype(F32)).astype(BF)

    def combine(lo, hi):
        rows = ret[lo:hi, :]
        part = jnp.dot(wt_hi[:, lo:hi], rows, preferred_element_type=F32) + jnp.dot(
            wt_lo[:, lo:hi], rows, preferred_element_type=F32
        )
        sh_acc[...] += part[0:TOK, :]

    gathers = {f"R{c}": g for c, g in enumerate(rows_g)} | {f"H{c}": g for c, g in enumerate(hid_g)}

    def wait_halo():
        halo_all().wait_recv()

    def finish():
        out_ref[...] = sh_acc[...].astype(BF)
        for cp in ends:
            cp.wait_send()

    calls = dict(
        zi=start_zin,
        halo=start_halo,
        cw=combine_weights,
        tq=turn_queries,
        tk=turn_keys,
        wh=wait_halo,
        wi=wait_zin,
        zo=start_zout,
        wo=wait_zout,
        at=attend,
        si=shared_in,
        so=shared_out,
        ei=experts_in,
        eo=experts_out,
        cb=combine,
        lda=lambda: wait_all(ld_att),
        lds=lambda: wait_all(ld_shared),
        ldb=lambda: wait_all(ld_big),
        end=finish,
    )
    for item in ORDER:
        with jax.named_scope(item):
            if item in gathers:
                gathers[item].next()
            else:
                name, _, arg = item.partition(":")
                calls[name](*[int(v) for v in arg.split("-") if v])


def deliver(a_in, b_in, a_out, b_out, sems):
    copies = [
        pltpu.make_async_copy(a_in, a_out, sems.at[0]),
        pltpu.make_async_copy(b_in, b_out, sems.at[1]),
    ]
    for cp in copies:
        cp.start()
    for cp in copies:
        cp.wait()


def _tables():
    quarter = HEAD_DIM // 4
    freq = np.float32(ROTARY_BASE) ** (
        np.float32(-4.0) * np.arange(quarter, dtype=np.float32) / np.float32(HEAD_DIM)
    )
    freq = freq.astype(np.float32)
    sign = np.concatenate([-np.ones(quarter), np.ones(quarter)])

    def of(index):
        angle = (index.astype(np.float32)[:, None] * freq).astype(np.float32).astype(np.float64)
        angle = np.concatenate([angle, angle], axis=1)
        return np.cos(angle), np.sin(angle) * sign

    def put(pair, left):
        pads = [(0, 0), (0, 64)] if left else [(0, 0), (64, 0)]
        return np.stack([np.pad(v, pads) for v in pair]).astype(np.float32)

    rows = put(of(np.arange(-2, 270)), True)
    cols = put(of(np.arange(GRID_W)), False)
    return rows, cols


ROW_TABLE, COL_TABLE = _tables()


def shards(
    query_vectors,
    key_vectors,
    value_vectors,
    query_gain,
    key_gain,
    sink_logits,
    moe_rows,
    norm_gain,
    expert_ids,
    route_weights,
    expert_gate,
    expert_up,
    expert_down,
    shared_gate,
    shared_up,
    shared_down,
):
    vm = pl.BlockSpec(memory_space=pltpu.VMEM)
    hb = pl.BlockSpec(memory_space=pl.ANY)
    dma = pltpu.SemaphoreType.DMA
    made = pl.pallas_call(
        kernel,
        out_shape=(
            jax.ShapeDtypeStruct((LEN, 2 * HEAD_DIM), BF),
            jax.ShapeDtypeStruct((TOK, FEAT), BF),
        ),
        in_specs=[hb] * 18,
        out_specs=(vm, vm),
        scratch_shapes=[
            pltpu.VMEM((TOP_K, TOK), jnp.int32),
            pltpu.VMEM((TOP_K, TOK), F32),
            pltpu.VMEM((LEN, 2 * HEAD_DIM), BF),
            pltpu.VMEM((1, HEAD_DIM), F32),
            pltpu.VMEM((1, HEAD_DIM), F32),
            pltpu.SMEM((2,), F32),
            pltpu.VMEM((1, D), F32),
            pltpu.VMEM((2, GRID_W, HEAD_DIM), F32),
            pltpu.VMEM((32, D), BF),
            pltpu.VMEM((32, D), BF),
            pltpu.VMEM((4, 4, PACKED + TOK, FEAT), BF),
            pltpu.VMEM((4, 4, PACKED + PACK, UNITS), BF),
            pltpu.VMEM((D, 2 * UNITS), BF),
            pltpu.VMEM((16 * UNITS, FEAT), BF),
            pltpu.VMEM((16, 128, FEAT), BF),
            pltpu.VMEM((2, 16, 128), F32),
            pltpu.VMEM((LEN + 2 * WINDOW, HEAD_DIM), BF),
            pltpu.VMEM((LEN + 2 * WINDOW, HEAD_DIM), BF),
            pltpu.VMEM((2, LEN, HEAD_DIM), BF),
            pltpu.VMEM((LEN + 2 * WINDOW, HEAD_DIM), BF),
            pltpu.VMEM((TPAD, FEAT), BF),
            pltpu.VMEM((8, TPAD), jnp.int32),
            pltpu.VMEM((8, TPAD), F32),
            pltpu.VMEM((ROWS, FEAT), BF),
            pltpu.VMEM((TPAD, ROWS), BF),
            pltpu.VMEM((TPAD, ROWS), BF),
            pltpu.VMEM((16, CHUNK, FEAT), BF),
            pltpu.VMEM((ROWS, FEAT), BF),
            pltpu.VMEM((ROWS, FEAT), BF),
            pltpu.VMEM((CHUNK, 128), F32),
            pltpu.VMEM((TOK, FEAT), F32),
            pltpu.VMEM((ROWS, FEAT), BF),
            pltpu.VMEM((120, 128), BF),
            pltpu.VMEM((128, 120), BF),
            dma((2 * NGATHER,)),
            dma((8 * NGATHER,)),
            dma((NCHUNK,)),
            dma((NCHUNK,)),
            dma((NCHUNK,)),
            dma((NCHUNK,)),
            dma((2,)),
            dma((22,)),
        ],
        compiler_params=pltpu.CompilerParams(
            collective_id=0, has_side_effects=True, vmem_limit_bytes=67043328
        ),
        name="fused",
    )(
        moe_rows,
        expert_ids.T,
        route_weights.T,
        query_vectors,
        key_vectors,
        value_vectors,
        query_gain.reshape(1, HEAD_DIM),
        key_gain.reshape(1, HEAD_DIM),
        sink_logits,
        norm_gain.reshape(1, D),
        jnp.asarray(COL_TABLE),
        jnp.asarray(ROW_TABLE),
        expert_gate,
        expert_up,
        expert_down,
        shared_gate.T,
        shared_up.T,
        shared_down.reshape(16, 32, FEAT),
    )
    return pl.pallas_call(
        deliver,
        out_shape=tuple(jax.ShapeDtypeStruct(v.shape, v.dtype) for v in made),
        in_specs=[vm, vm],
        out_specs=(hb, hb),
        scratch_shapes=[dma((2,))],
        name="deliver",
    )(*made)


def solution(mesh):
    placed = (
        P("ep", "tp"),
        P("ep", "tp"),
        P("ep", "tp"),
        P(),
        P(),
        P("tp"),
        P("ep", "tp"),
        P(),
        P("ep", None),
        P("ep", None),
        P("ep", None, "tp"),
        P("ep", None, "tp"),
        P("ep", None, "tp"),
        P(None, "tp"),
        P(None, "tp"),
        P(None, "tp"),
    )
    return jax.shard_map(
        shards,
        mesh=mesh,
        in_specs=placed,
        out_specs=(P("ep", "tp"), P("ep", "tp")),
        check_vma=False,
    )
```

```python
import numpy as np
import jax
import jax.numpy as jnp
from jax import lax
from jax.experimental import pallas as pl
from jax.experimental.pallas import tpu as pltpu
from jax.sharding import PartitionSpec as P

MESH = pl.DeviceIdType.MESH
BF = jnp.bfloat16
F32 = jnp.float32

HEAD_DIM = 128
WINDOW = 128
GRID_W = 64
D = 4096
TOP_K = 4
EPS = 1e-06
ROTARY_BASE = 10000.0

NZ = 16
TOK = 160
TPAD = 256
SLOT = 32
ROWS = 32 * SLOT
LEN = 512
FEAT = 256
UNITS = 128
PACK = 40

GROUPS = [[1, -1], [5, -5], [6, -6], [8], [7, -7], [4, -4], [0], [3, -3], [2, -2]]
REL = sum(GROUPS, [])
NCHUNK = len(GROUPS)
ZFIRST = [2 * SLOT * sum(len(g) for g in GROUPS[:c]) for c in range(NCHUNK)]
ZSIZE = [2 * SLOT * len(g) for g in GROUPS]
SIZE = [(60 * len(g) + 7) // 8 * 8 for g in GROUPS]
FIRST = [sum(SIZE[:c]) for c in range(NCHUNK)]
PACKED = sum(SIZE)
HERE = REL.index(0)
OWN_CHUNK = [c for c in range(NCHUNK) if 0 in GROUPS[c]][0]


def _inv(p):
    return REL.index(REL[p] if REL[p] in (0, 8) else -REL[p])


INV = [_inv(p) for p in range(NZ)]
CHUNK = 256

GATHER_1 = list(zip(FIRST, SIZE)) + [(PACKED, TOK)]
GATHER_2 = list(zip(FIRST, SIZE)) + [(PACKED, PACK)]
NGATHER = NCHUNK + 1

ORDER = (
    "R9", "zi:0", "halo", "zi:1", "zi:2", "zi:3", "zi:4", "zi:5", "zi:6", "zi:7", "zi:8",
    "cw", "lda", "lds", "ldb", "wi:6", "R6", "wi:0", "R0", "tq", "R9", "R6", "wh", "tk",
    "R0", "at:0", "R9", "wi:1", "R1", "R0", "R6", "at:1", "R9", "R1", "R0", "wi:2", "R2",
    "R9", "si", "H9", "R1", "R6", "wi:3", "R3", "R2", "R0", "ei:0", "H0", "R1", "R3", "R2",
    "wi:4", "R4", "H9", "H0", "R6", "ei:6", "H6", "R1", "ei:1", "H1", "R2", "R3", "R4",
    "wi:5", "R5", "H9", "H0", "H1", "wi:7", "R7", "R2", "ei:2", "H2", "R3", "R4", "R5",
    "H9", "H0", "H1", "R7", "H2", "R3", "ei:3", "H3", "R4", "R5", "wi:8", "R8", "H9", "so",
    "H1", "H0", "eo:0", "zo:0", "R7", "H2", "H3", "at:2", "R4", "ei:4", "H4", "R5", "H1",
    "eo:1", "zo:1", "H3", "R7", "H2", "R8", "H4", "at:3", "R5", "ei:5", "H5", "H3", "R7",
    "ei:7", "H7", "H2", "eo:2", "zo:2", "R8", "H4", "H5", "H3", "eo:3", "zo:3", "R8", "H4",
    "H5", "H6", "H7", "wo:0", "cb:0-128", "wo:1", "cb:128-256", "R8", "ei:8", "H8", "H4",
    "eo:4", "zo:4", "H5", "H6", "H7", "wo:2", "cb:256-384", "H8", "H5", "eo:5", "zo:5",
    "H6", "H8", "H7", "H6", "eo:6", "zo:6", "H8", "H7", "eo:7", "zo:7", "H8", "eo:8",
    "zo:8", "wo:3", "wo:4", "cb:384-512", "wo:5", "cb:512-640", "wo:6", "cb:640-768",
    "wo:7", "cb:768-896", "wo:8", "cb:896-1024", "end",
)


def up8(v):
    return (v + 7) // 8 * 8


def kernel(
    x_hbm,
    ids_hbm,
    rw_hbm,
    q_hbm,
    k_hbm,
    v_hbm,
    qg_hbm,
    kg_hbm,
    sink_hbm,
    ng_hbm,
    colt_hbm,
    rowt_hbm,
    gate_hbm,
    up_hbm,
    down_hbm,
    sg_hbm,
    su_hbm,
    sd_hbm,
    att_ref,
    out_ref,
    ids_ref,
    rw_ref,
    q_ref,
    qg_ref,
    kg_ref,
    sink_ref,
    ng_ref,
    colt_ref,
    sg_ref,
    su_ref,
    xg,
    hg,
    wgu,
    wd,
    wsd,
    rowt,
    kpad,
    vpad,
    qt,
    kt,
    xpad,
    idsp,
    rwp,
    send,
    wt_hi,
    wt_lo,
    lhs,
    res,
    ret,
    acc,
    sh_acc,
    zst,
    pick,
    spread,
    g_send,
    g_recv,
    zi_send,
    zi_recv,
    zo_send,
    zo_recv,
    halo_sem,
    loc,
):
    ep = lax.axis_index("ep")
    tp = lax.axis_index("tp")
    z = ep // 2
    core = ep % 2
    y = tp // 4
    x = tp % 4
    xr, xl = (x + 1) % 4, (x + 3) % 4
    yr, yl = (y + 1) % 4, (y + 3) % 4
    xo, yo = (x + 2) % 4, (y + 2) % 4

    def ep_at(rel, c):
        return ((z + rel + NZ) % NZ) * 2 + c

    ep_hi = (ep + 1) % 32
    ep_lo = (ep + 31) % 32

    barrier = pltpu.get_barrier_semaphore()
    for p in range(NZ):
        for c in range(2):
            if REL[p] == 0:
                continue
            pl.semaphore_signal(
                barrier, inc=1, device_id={"ep": ep_at(REL[p], c), "tp": tp}, device_id_type=MESH
            )
    pl.semaphore_signal(
        barrier, inc=1, device_id={"ep": z * 2 + (1 - core), "tp": tp}, device_id_type=MESH
    )
    plane = [y * 4 + xr, y * 4 + xl, yr * 4 + x, yl * 4 + x]
    for t in plane:
        pl.semaphore_signal(barrier, inc=1, device_id={"ep": ep, "tp": t}, device_id_type=MESH)

    def load(i, src, dst):
        cp = pltpu.make_async_copy(src, dst, loc.at[i])
        cp.start()
        return cp

    mid = pl.ds(WINDOW, LEN)
    rows_at = pl.ds(PACKED, TOK)
    ld_own = load(0, x_hbm, xg.at[y, x, rows_at])
    ld_route = [
        load(1, ids_hbm, ids_ref),
        load(2, rw_hbm, rw_ref),
        load(3, x_hbm, xpad.at[pl.ds(0, TOK)]),
    ]
    ld_kv = [load(4, k_hbm, kpad.at[mid]), load(5, v_hbm, vpad.at[mid])]
    ld_att = [
        load(6, q_hbm, q_ref),
        load(7, qg_hbm, qg_ref),
        load(8, kg_hbm, kg_ref),
        load(9, sink_hbm, sink_ref),
        load(10, colt_hbm, colt_ref),
        load(11, rowt_hbm.at[:, pl.ds(pl.multiple_of(ep * 8, 8), 16), :], rowt),
    ]
    ld_shared = [load(12, sg_hbm, sg_ref), load(13, su_hbm, su_ref), load(14, ng_hbm, ng_ref)] + [
        load(15 + j, sd_hbm, wsd.at[:, pl.ds(32 * j, 32), :]) for j in range(4)
    ]
    ld_big = [
        load(19, gate_hbm.at[0], wgu.at[:, 0:128]),
        load(20, up_hbm.at[0], wgu.at[:, 128:256]),
        load(21, down_hbm.at[0], wd),
    ]

    def wait_all(copies):
        for cp in copies:
            cp.wait()

    xpad[TOK:TPAD, :] = jnp.zeros((TPAD - TOK, FEAT), BF)
    idsp[...] = jnp.full(idsp.shape, -1, jnp.int32)
    rwp[...] = jnp.zeros_like(rwp)
    wait_all(ld_route)
    idsp[0:TOP_K, 0:TOK] = ids_ref[...]
    rwp[0:TOP_K, 0:TOK] = rw_ref[...]

    row32 = lax.broadcasted_iota(jnp.int32, (32, TPAD), 0)
    pos32 = row32 >> 1
    rel32 = jnp.zeros((32, TPAD), jnp.int32)
    for p in range(NZ):
        rel32 = jnp.where(pos32 == p, REL[p] + NZ, rel32)
    expert32 = ((z + rel32) & (NZ - 1)) * 2 + (row32 & 1)
    named = jnp.zeros((32, TPAD), F32)
    weight = jnp.zeros((32, TPAD), F32)
    for k in range(TOP_K):
        same = idsp[k : k + 1, :] == expert32
        named = jnp.where(same, 1.0, named)
        weight = jnp.where(same, rwp[k : k + 1, :], weight)
    before = (
        lax.broadcasted_iota(jnp.int32, (TPAD, TPAD), 0)
        < lax.broadcasted_iota(jnp.int32, (TPAD, TPAD), 1)
    )
    count = jnp.dot(
        named.astype(BF), jnp.where(before, 1.0, 0.0).astype(BF), preferred_element_type=F32
    )
    slot32 = jnp.where(named > 0.5, count, -1.0)
    slot_row = lax.broadcasted_iota(jnp.int32, (SLOT, TPAD), 0).astype(F32)
    for t in range(NCHUNK):
        lo, n = ZFIRST[t], ZSIZE[t]
        picks = [
            jnp.where(slot32[i : i + 1, :] == slot_row, 1.0, 0.0).astype(BF)
            for i in range(lo // SLOT, (lo + n) // SLOT)
        ]
        send[lo : lo + n, :] = jnp.dot(
            jnp.concatenate(picks, axis=0), xpad[...], preferred_element_type=F32
        ).astype(BF)
    mine = pl.ds(pl.multiple_of(HERE * 2 * SLOT + core * SLOT, SLOT), SLOT)
    other = pl.ds(pl.multiple_of(HERE * 2 * SLOT + (1 - core) * SLOT, SLOT), SLOT)
    zst[mine, :] = send[mine, :]

    def moved(r):
        over = [jnp.where(r >= 30 * i, 2, 0) for i in (1, 2, 3)]
        return r + over[0] + over[1] + over[2]

    iota = lambda shape, axis: lax.broadcasted_iota(jnp.int32, shape, axis)
    wide_shape, tall_shape = (120, 128), (128, 120)
    pick[...] = jnp.where(
        moved(iota(wide_shape, 0)) == iota(wide_shape, 1), 1.0, 0.0
    ).astype(BF)
    spread[...] = jnp.where(
        iota(tall_shape, 0) == moved(iota(tall_shape, 1)), 1.0, 0.0
    ).astype(BF)

    def pack(c):
        rows = jnp.dot(
            pick[0 : SIZE[c], 0 : ZSIZE[c]],
            zst[ZFIRST[c] : ZFIRST[c] + ZSIZE[c], :],
            preferred_element_type=F32,
        )
        xg[y, x, FIRST[c] : FIRST[c] + SIZE[c], :] = rows.astype(BF)

    ld_own.wait()
    pl.semaphore_wait(barrier, 35)

    ends = []

    def remote(src, dst, ssem, rsem, dev):
        cp = pltpu.make_async_remote_copy(
            src_ref=src,
            dst_ref=dst,
            send_sem=ssem,
            recv_sem=rsem,
            device_id=dev,
            device_id_type=MESH,
        )
        return cp

    partner = {"ep": z * 2 + (1 - core), "tp": tp}

    class Gather:
        def __init__(self, which, buf, start, size, index):
            self.buf, self.width = buf, buf.shape[3]
            self.start, self.size = start, size
            self.index = which * NGATHER + index
            na = up8(size // 2)
            self.ranges = []
            for first, count in ((start, na), (start + na, size - na)):
                self.ranges.append((first, count, up8(count // 2)))
            self.stage = 0

        def next(self):
            s = self.stage
            self.stage += 1
            buf = self.buf
            ssem = g_send.at[self.index]
            if s > 0:
                rows = pl.ds(self.start, self.size)
                whole = (
                    buf.at[pl.ds(0, 2), 0, rows],
                    buf.at[0, 0, rows],
                    buf.at[pl.ds(0, 2), :, rows],
                    buf.at[0, :, rows],
                )[s - 1]
                rsem = g_recv.at[self.index * 3 + (s - 1) % 3]
                remote(whole, whole, ssem, rsem, partner).wait_recv()
            if s == 4:
                whole = lhs.at[pl.ds(0, 15), pl.ds(0, self.size), pl.ds(0, self.width)]
                ends.append(remote(whole, whole, ssem, g_recv.at[self.index * 3], partner))
                return
            near, wide = [], []
            for half, (first, count, low) in enumerate(self.ranges):
                full = pl.ds(first, count)
                part_lo, part_hi = pl.ds(first, low), pl.ds(first + low, count - low)
                if half == 0:
                    piece = lambda w, v, r: buf.at[w, v, r]
                    group = lambda w, r: buf.at[w, :, r]
                    n_me, n_r, n_l, n_o, w_me, w_r, w_l = x, xr, xl, xo, y, yr, yl
                    to_n, to_w = (y * 4 + xr, y * 4 + xl), (yr * 4 + x, yl * 4 + x)
                else:
                    piece = lambda w, v, r: buf.at[v, w, r]
                    group = lambda w, r: buf.at[:, w, r]
                    n_me, n_r, n_l, n_o, w_me, w_r, w_l = y, yr, yl, yo, x, xr, xl
                    to_n, to_w = (yr * 4 + x, yl * 4 + x), (y * 4 + xr, y * 4 + xl)
                if s == 0:
                    near += [(piece(w_me, n_me, full), to, 0) for to in to_n]
                    wide += [(piece(w_me, n_me, full), to, 2) for to in to_w]
                elif s == 1:
                    near += [
                        (piece(w_me, n_l, part_lo), to_n[0], 1),
                        (piece(w_me, n_r, part_hi), to_n[1], 1),
                    ]
                    wide += [(piece(w_me, v, full), to, 2) for v in (n_l, n_r) for to in to_w]
                elif s == 2:
                    wide += [(piece(w_me, n_o, full), to, 2) for to in to_w]
                else:
                    wide += [
                        (group(w_l, part_lo), to_w[0], 3),
                        (group(w_r, part_hi), to_w[1], 3),
                    ]
            for ref, to, kind in near + wide:
                remote(
                    ref, ref, ssem, g_recv.at[self.index * 3 + kind % 3], {"ep": ep, "tp": to}
                ).start()

    rows_g = [Gather(0, xg, s, n, i) for i, (s, n) in enumerate(GATHER_1)]
    hid_g = [Gather(1, hg, s, n, i) for i, (s, n) in enumerate(GATHER_2)]

    def z_start(chunk, src_at, dst_at, ssem, rsem):
        for p in range(ZFIRST[chunk] // (2 * SLOT), (ZFIRST[chunk] + ZSIZE[chunk]) // (2 * SLOT)):
            q = INV[p]
            back = pl.ds(pl.multiple_of(q * 2 * SLOT + core * SLOT, SLOT), SLOT)
            if REL[p] == 0:
                pieces = [(other, partner)]
            else:
                pieces = [
                    (
                        pl.ds(p * 2 * SLOT + c * SLOT, SLOT),
                        {"ep": ep_at(REL[p], c), "tp": tp},
                    )
                    for c in range(2)
                ]
            for rows, dev in pieces:
                remote(src_at(rows), dst_at(back), ssem.at[0], rsem.at[chunk], dev).start()

    def z_wait(chunk, at, rsem, ssem):
        rows = other if chunk == OWN_CHUNK else pl.ds(ZFIRST[chunk], ZSIZE[chunk])
        remote(at(rows), at(rows), ssem.at[0], rsem.at[chunk], partner).wait_recv()

    own_at = lambda r: zst.at[r]
    send_at = lambda r: send.at[r]
    res_at = lambda r: res.at[r]
    ret_at = lambda r: ret.at[r]

    def start_zin(chunk):
        z_start(chunk, send_at, own_at, zi_send, zi_recv)

    def wait_zin(chunk):
        z_wait(chunk, own_at, zi_recv, zi_send)
        pack(chunk)

    def start_zout(chunk):
        z_start(chunk, res_at, ret_at, zo_send, zo_recv)

    def wait_zout(chunk):
        z_wait(chunk, ret_at, zo_recv, zo_send)

    def start_halo():
        tail, head = pl.ds(LEN, WINDOW), pl.ds(WINDOW, WINDOW)
        wait_all(ld_kv)
        for i, pad in enumerate((kpad, vpad)):
            for j, (part, to, at) in enumerate(
                ((tail, ep_hi, pl.ds(0, WINDOW)), (head, ep_lo, pl.ds(WINDOW + LEN, WINDOW)))
            ):
                cp = remote(
                    pad.at[part],
                    pad.at[at],
                    halo_sem.at[0],
                    halo_sem.at[1],
                    {"ep": to, "tp": tp},
                )
                cp.start()
        ends.append(halo_all())

    def halo_all():
        ref = kpad.at[pl.ds(0, 4 * WINDOW)]
        return remote(ref, ref, halo_sem.at[0], halo_sem.at[1], partner)

    first_half = (lax.broadcasted_iota(jnp.int32, (GRID_W, HEAD_DIM), 1) & 63) < 32

    def turn(raw, gain, g):
        f = raw.astype(F32)
        n = f * lax.rsqrt(jnp.mean(f * f, axis=-1, keepdims=True) + EPS) * gain
        other = jnp.where(first_half, pltpu.roll(n, 96, 1), pltpu.roll(n, 32, 1))
        cos = rowt[0, pl.ds(g, 1), :] + colt_ref[0]
        sin = rowt[1, pl.ds(g, 1), :] + colt_ref[1]
        return (n * cos + other * sin).astype(BF)

    def turn_queries():
        for g in range(LEN // GRID_W):
            for h in range(2):
                rows = slice(g * GRID_W, (g + 1) * GRID_W)
                qt[h, rows, :] = turn(
                    q_ref[rows, h * HEAD_DIM : (h + 1) * HEAD_DIM], qg_ref[...], g + 2
                )

    def turn_keys():
        for g in range((LEN + 2 * WINDOW) // GRID_W):
            rows = slice(g * GRID_W, (g + 1) * GRID_W)
            kt[rows, :] = turn(kpad[rows, :], kg_ref[...], g)

    near_q = lax.broadcasted_iota(jnp.int32, (128, 384), 0)
    near_k = lax.broadcasted_iota(jnp.int32, (128, 384), 1)

    def attend(b):
        key_pos = near_k + (ep * LEN - WINDOW + 128 * b)
        inside = (
            (near_k >= near_q)
            & (near_k <= near_q + 2 * WINDOW)
            & (key_pos >= 0)
            & (key_pos < 32 * LEN)
        )
        keys = kt[128 * b : 128 * b + 384, :]
        values = vpad[128 * b : 128 * b + 384, :]
        for h in range(2):
            scores = lax.dot_general(
                qt[h, 128 * b : 128 * b + 128, :],
                keys,
                (((1,), (1,)), ((), ())),
                preferred_element_type=F32,
            ) * (HEAD_DIM ** (-0.5))
            raised = jnp.where(inside, jnp.exp(scores), 0.0)
            sink = jnp.exp(jnp.full((128, 1), sink_ref[h], F32))
            den = sink + jnp.sum(raised, axis=-1, keepdims=True)
            weights = (raised * (1.0 / den)).astype(BF)
            mixed = jnp.dot(weights, values, preferred_element_type=F32)
            att_ref[128 * b : 128 * b + 128, h * 128 : (h + 1) * 128] = mixed.astype(BF)

    def scale_rows(start, size):
        acc[0:size, 0:128] = jnp.zeros((size, 128), F32)

        def one(s, carry):
            f = xg[s // 4, s % 4, start : start + size, :].astype(F32)
            sq = f * f
            acc[0:size, 0:128] += sq[:, 0:128] + sq[:, 128:256]
            lhs[s, 0:size, :] = (f * ng_ref[:, pl.ds(pl.multiple_of(s * FEAT, FEAT), FEAT)]).astype(BF)
            return carry

        lax.fori_loop(0, 16, one, 0)
        return lax.rsqrt(jnp.sum(acc[0:size, 0:128], axis=-1, keepdims=True) / D + EPS)

    def activate(g, u, factor):
        g, u = g * factor, u * factor
        return (g / (1.0 + jnp.exp(-g)) * u).astype(BF)

    def experts_in(c):
        start, size = FIRST[c], SIZE[c]
        factor = scale_rows(start, size)
        both = jnp.dot(
            jnp.concatenate([lhs[s, 0:size, :] for s in range(16)], axis=1),
            wgu[...],
            preferred_element_type=F32,
        )
        hg[y, x, start : start + size, :] = activate(both[:, 0:128], both[:, 128:256], factor)

    def shared_in():
        factor = scale_rows(PACKED, TOK)
        rows = jnp.concatenate([lhs[s, 0:TOK, :] for s in range(16)], axis=1)
        across = (((1,), (1,)), ((), ()))
        g = lax.dot_general(rows, sg_ref[...], across, preferred_element_type=F32)
        u = lax.dot_general(rows, su_ref[...], across, preferred_element_type=F32)
        h = activate(g, u, factor).astype(F32)
        packed = jnp.concatenate([h[40 * j : 40 * j + 40, :] for j in range(4)], axis=1)
        hg[y, x, PACKED : PACKED + PACK, :] = packed.astype(BF)

    def experts_out(c):
        start, size = FIRST[c], SIZE[c]
        rows = jnp.concatenate(
            [hg[s // 4, s % 4, start : start + size, :] for s in range(16)], axis=1
        )
        packed = jnp.dot(rows, wd[...], preferred_element_type=F32).astype(BF)
        res[ZFIRST[c] : ZFIRST[c] + ZSIZE[c], :] = jnp.dot(
            spread[0 : ZSIZE[c], 0:size], packed, preferred_element_type=F32
        ).astype(BF)
        if c == OWN_CHUNK:
            ret[mine, :] = res[mine, :]

    def shared_out():
        group = lax.broadcasted_iota(jnp.int32, (40, 128), 1) // 32
        total = jnp.zeros((TOK, FEAT), F32)
        for s in range(16):
            piece = hg[s // 4, s % 4, PACKED : PACKED + PACK, :].astype(F32)[0:40, :]
            parts = jnp.concatenate(
                [jnp.where(group == j, piece, 0.0) for j in range(4)], axis=0
            )
            total += jnp.dot(parts.astype(BF), wsd[s], preferred_element_type=F32)
        sh_acc[...] = total

    def combine_weights():
        for t in range(ROWS // CHUNK):
            full = jnp.concatenate(
                [
                    jnp.where(slot32[i : i + 1, :] == slot_row, weight[i : i + 1, :], 0.0)
                    for i in range(8 * t, 8 * t + 8)
                ],
                axis=0,
            )
            turned = jnp.transpose(full)
            high = turned.astype(BF)
            rows = slice(t * CHUNK, (t + 1) * CHUNK)
            wt_hi[:, rows] = high
            wt_lo[:, rows] = (turned - high.astype(F32)).astype(BF)

    def combine(lo, hi):
        rows = ret[lo:hi, :]
        part = jnp.dot(wt_hi[:, lo:hi], rows, preferred_element_type=F32) + jnp.dot(
            wt_lo[:, lo:hi], rows, preferred_element_type=F32
        )
        sh_acc[...] += part[0:TOK, :]

    gathers = {f"R{c}": g for c, g in enumerate(rows_g)} | {f"H{c}": g for c, g in enumerate(hid_g)}

    def wait_halo():
        halo_all().wait_recv()

    def finish():
        most = pl.ds(0, ROWS - SLOT)
        ends.append(remote(send.at[most], send.at[most], zi_send.at[0], zi_recv.at[0], partner))
        ends.append(remote(res.at[most], res.at[most], zo_send.at[0], zo_recv.at[0], partner))
        out_ref[...] = sh_acc[...].astype(BF)
        for cp in ends:
            cp.wait_send()

    calls = dict(
        zi=start_zin,
        halo=start_halo,
        cw=combine_weights,
        tq=turn_queries,
        tk=turn_keys,
        wh=wait_halo,
        wi=wait_zin,
        zo=start_zout,
        wo=wait_zout,
        at=attend,
        si=shared_in,
        so=shared_out,
        ei=experts_in,
        eo=experts_out,
        cb=combine,
        lda=lambda: wait_all(ld_att),
        lds=lambda: wait_all(ld_shared),
        ldb=lambda: wait_all(ld_big),
        end=finish,
    )
    for item in ORDER:
        with jax.named_scope(item):
            if item in gathers:
                gathers[item].next()
            else:
                name, _, arg = item.partition(":")
                calls[name](*[int(v) for v in arg.split("-") if v])


def deliver(a_in, b_in, a_out, b_out, sems):
    copies = [
        pltpu.make_async_copy(a_in, a_out, sems.at[0]),
        pltpu.make_async_copy(b_in, b_out, sems.at[1]),
    ]
    for cp in copies:
        cp.start()
    for cp in copies:
        cp.wait()


def _tables():
    quarter = HEAD_DIM // 4
    freq = np.float32(ROTARY_BASE) ** (
        np.float32(-4.0) * np.arange(quarter, dtype=np.float32) / np.float32(HEAD_DIM)
    )
    freq = freq.astype(np.float32)
    sign = np.concatenate([-np.ones(quarter), np.ones(quarter)])

    def of(index):
        angle = (index.astype(np.float32)[:, None] * freq).astype(np.float32).astype(np.float64)
        angle = np.concatenate([angle, angle], axis=1)
        return np.cos(angle), np.sin(angle) * sign

    def put(pair, left):
        pads = [(0, 0), (0, 64)] if left else [(0, 0), (64, 0)]
        return np.stack([np.pad(v, pads) for v in pair]).astype(np.float32)

    rows = put(of(np.arange(-2, 270)), True)
    cols = put(of(np.arange(GRID_W)), False)
    return rows, cols


ROW_TABLE, COL_TABLE = _tables()


def shards(
    query_vectors,
    key_vectors,
    value_vectors,
    query_gain,
    key_gain,
    sink_logits,
    moe_rows,
    norm_gain,
    expert_ids,
    route_weights,
    expert_gate,
    expert_up,
    expert_down,
    shared_gate,
    shared_up,
    shared_down,
):
    vm = pl.BlockSpec(memory_space=pltpu.VMEM)
    hb = pl.BlockSpec(memory_space=pl.ANY)
    dma = pltpu.SemaphoreType.DMA
    made = pl.pallas_call(
        kernel,
        out_shape=(
            pltpu.VMEM((LEN, 2 * HEAD_DIM), BF),
            pltpu.VMEM((TOK, FEAT), BF),
        ),
        in_specs=[hb] * 18,
        out_specs=(vm, vm),
        scratch_shapes=[
            pltpu.VMEM((TOP_K, TOK), jnp.int32),
            pltpu.VMEM((TOP_K, TOK), F32),
            pltpu.VMEM((LEN, 2 * HEAD_DIM), BF),
            pltpu.VMEM((1, HEAD_DIM), F32),
            pltpu.VMEM((1, HEAD_DIM), F32),
            pltpu.SMEM((2,), F32),
            pltpu.VMEM((1, D), F32),
            pltpu.VMEM((2, GRID_W, HEAD_DIM), F32),
            pltpu.VMEM((32, D), BF),
            pltpu.VMEM((32, D), BF),
            pltpu.VMEM((4, 4, PACKED + TOK, FEAT), BF),
            pltpu.VMEM((4, 4, PACKED + PACK, UNITS), BF),
            pltpu.VMEM((D, 2 * UNITS), BF),
            pltpu.VMEM((16 * UNITS, FEAT), BF),
            pltpu.VMEM((16, 128, FEAT), BF),
            pltpu.VMEM((2, 16, 128), F32),
            pltpu.VMEM((LEN + 2 * WINDOW, HEAD_DIM), BF),
            pltpu.VMEM((LEN + 2 * WINDOW, HEAD_DIM), BF),
            pltpu.VMEM((2, LEN, HEAD_DIM), BF),
            pltpu.VMEM((LEN + 2 * WINDOW, HEAD_DIM), BF),
            pltpu.VMEM((TPAD, FEAT), BF),
            pltpu.VMEM((8, TPAD), jnp.int32),
            pltpu.VMEM((8, TPAD), F32),
            pltpu.VMEM((ROWS, FEAT), BF),
            pltpu.VMEM((TPAD, ROWS), BF),
            pltpu.VMEM((TPAD, ROWS), BF),
            pltpu.VMEM((16, CHUNK, FEAT), BF),
            pltpu.VMEM((ROWS, FEAT), BF),
            pltpu.VMEM((ROWS, FEAT), BF),
            pltpu.VMEM((CHUNK, 128), F32),
            pltpu.VMEM((TOK, FEAT), F32),
            pltpu.VMEM((ROWS, FEAT), BF),
            pltpu.VMEM((120, 128), BF),
            pltpu.VMEM((128, 120), BF),
            dma((2 * NGATHER,)),
            dma((6 * NGATHER,)),
            dma((1,)),
            dma((NCHUNK,)),
            dma((1,)),
            dma((NCHUNK,)),
            dma((2,)),
            dma((22,)),
        ],
        compiler_params=pltpu.CompilerParams(
            collective_id=0, has_side_effects=True, vmem_limit_bytes=66600000
        ),
        name="fused",
    )(
        moe_rows,
        expert_ids.T,
        route_weights.T,
        query_vectors,
        key_vectors,
        value_vectors,
        query_gain.reshape(1, HEAD_DIM),
        key_gain.reshape(1, HEAD_DIM),
        sink_logits,
        norm_gain.reshape(1, D),
        jnp.asarray(COL_TABLE),
        jnp.asarray(ROW_TABLE),
        expert_gate,
        expert_up,
        expert_down,
        shared_gate.T,
        shared_up.T,
        shared_down.reshape(16, 32, FEAT),
    )
    return pl.pallas_call(
        deliver,
        out_shape=tuple(jax.ShapeDtypeStruct(v.shape, v.dtype) for v in made),
        in_specs=[vm, vm],
        out_specs=(hb, hb),
        scratch_shapes=[dma((2,))],
        compiler_params=pltpu.CompilerParams(vmem_limit_bytes=2 * 1024 * 1024),
        name="deliver",
    )(*made)


def solution(mesh):
    placed = (
        P("ep", "tp"),
        P("ep", "tp"),
        P("ep", "tp"),
        P(),
        P(),
        P("tp"),
        P("ep", "tp"),
        P(),
        P("ep", None),
        P("ep", None),
        P("ep", None, "tp"),
        P("ep", None, "tp"),
        P("ep", None, "tp"),
        P(None, "tp"),
        P(None, "tp"),
        P(None, "tp"),
    )
    return jax.shard_map(
        shards,
        mesh=mesh,
        in_specs=placed,
        out_specs=(P("ep", "tp"), P("ep", "tp")),
        check_vma=False,
    )
```

```python
import numpy as np
import jax
import jax.numpy as jnp
from jax import lax
from jax.experimental import pallas as pl
from jax.experimental.pallas import tpu as pltpu
from jax.sharding import PartitionSpec as P

MESH = pl.DeviceIdType.MESH
BF = jnp.bfloat16
F32 = jnp.float32

HEAD_DIM = 128
WINDOW = 128
GRID_W = 64
D = 4096
TOP_K = 4
EPS = 1e-06
ROTARY_BASE = 10000.0

NZ = 16
TOK = 160
TPAD = 256
SLOT = 32
ROWS = 32 * SLOT
LEN = 512
FEAT = 256
UNITS = 128
PACK = 40

GROUPS = [[3, -3], [8], [5, -5], [6, -6], [7, -7], [0], [4, -4], [2, -2], [1, -1]]
REL = sum(GROUPS, [])
NCHUNK = len(GROUPS)
ZFIRST = [2 * SLOT * sum(len(g) for g in GROUPS[:c]) for c in range(NCHUNK)]
ZSIZE = [2 * SLOT * len(g) for g in GROUPS]
SIZE = [(60 * len(g) + 7) // 8 * 8 for g in GROUPS]
FIRST = [sum(SIZE[:c]) for c in range(NCHUNK)]
PACKED = sum(SIZE)
HERE = REL.index(0)
OWN_CHUNK = [c for c in range(NCHUNK) if 0 in GROUPS[c]][0]


def _inv(p):
    return REL.index(REL[p] if REL[p] in (0, 8) else -REL[p])


INV = [_inv(p) for p in range(NZ)]
CHUNK = 256

GATHER_1 = list(zip(FIRST, SIZE)) + [(PACKED, TOK)]
GATHER_2 = list(zip(FIRST, SIZE)) + [(PACKED, PACK)]
NGATHER = NCHUNK + 1

ORDER = (
    "R9", "zi:0", "halo", "zi:1", "zi:2", "zi:3", "zi:4", "zi:5", "zi:6", "zi:7", "zi:8",
    "go", "cw", "lda", "tq", "wi:5", "R5", "R9", "wh", "tk", "at:0", "R5", "wi:0", "R0",
    "at:1", "at:2", "at:3", "R9", "R0", "R5", "R9", "R0", "wi:1", "R1", "R5", "wi:2", "R2",
    "R9", "lds", "si", "H9", "R0", "R1", "R5", "ldb", "ei:5", "H5", "R2", "H9", "wi:3",
    "R3", "R0", "ei:0", "H0", "H5", "R2", "R1", "H9", "R3", "H0", "wi:4", "R4", "H5", "R2",
    "H9", "R3", "R1", "H0", "R4", "H5", "R2", "ei:2", "H2", "H9", "so", "R4", "H0", "R3",
    "wi:6", "R6", "R1", "ei:1", "H1", "H5", "eo:5", "zo:5", "H2", "wi:7", "R7", "R4", "H0",
    "eo:0", "zo:0", "wi:8", "R8", "R3", "ei:3", "H3", "H1", "H2", "R6", "R7", "R4", "ei:4",
    "H4", "H3", "H1", "R8", "wo:0", "cb:0-128", "H2", "R6", "R7", "H4", "H3", "H1", "R8",
    "H2", "eo:2", "zo:2", "R6", "R7", "H4", "H3", "H1", "eo:1", "zo:1", "R8", "R6", "ei:6",
    "H6", "H4", "R7", "ei:7", "H7", "H3", "eo:3", "zo:3", "H6", "R8", "ei:8", "H8", "H7",
    "H4", "eo:4", "zo:4", "H6", "H8", "H7", "H6", "H8", "wo:1", "wo:2", "cb:128-256", "H7",
    "H6", "eo:6", "zo:6", "H8", "H7", "eo:7", "zo:7", "wo:3", "cb:256-384", "H8", "eo:8",
    "zo:8", "wo:4", "cb:384-512", "wo:5", "cb:512-640", "wo:6", "cb:640-768", "wo:7",
    "cb:768-896", "wo:8", "cb:896-1024", "end",
)


def up8(v):
    return (v + 7) // 8 * 8


def kernel(
    x_hbm,
    ids_hbm,
    rw_hbm,
    q_hbm,
    k_hbm,
    v_hbm,
    qg_hbm,
    kg_hbm,
    sink_hbm,
    ng_hbm,
    colt_hbm,
    rowt_hbm,
    gate_hbm,
    up_hbm,
    down_hbm,
    sg_hbm,
    su_hbm,
    sd_hbm,
    att_ref,
    out_ref,
    ids_ref,
    rw_ref,
    q_ref,
    qg_ref,
    kg_ref,
    sink_ref,
    ng_ref,
    colt_ref,
    sg_ref,
    su_ref,
    xg,
    hg,
    wgu,
    wd,
    wsd,
    rowt,
    kpad,
    vpad,
    qt,
    kt,
    xpad,
    idsp,
    rwp,
    send,
    wt_hi,
    wt_lo,
    lhs,
    res,
    ret,
    acc,
    sh_acc,
    zst,
    pick,
    spread,
    g_send,
    g_recv,
    zi_send,
    zi_recv,
    zo_send,
    zo_recv,
    halo_sem,
    loc,
):
    ep = lax.axis_index("ep")
    tp = lax.axis_index("tp")
    z = ep // 2
    core = ep % 2
    y = tp // 4
    x = tp % 4
    xr, xl = (x + 1) % 4, (x + 3) % 4
    yr, yl = (y + 1) % 4, (y + 3) % 4
    xo, yo = (x + 2) % 4, (y + 2) % 4

    def ep_at(rel, c):
        return ((z + rel + NZ) % NZ) * 2 + c

    ep_hi = (ep + 1) % 32
    ep_lo = (ep + 31) % 32

    barrier = pltpu.get_barrier_semaphore()
    for rel in sorted(REL, key=abs, reverse=True)[:-1]:
        for c in range(2):
            pl.semaphore_signal(
                barrier, inc=1, device_id={"ep": ep_at(rel, c), "tp": tp}, device_id_type=MESH
            )
    pl.semaphore_signal(
        barrier, inc=1, device_id={"ep": z * 2 + (1 - core), "tp": tp}, device_id_type=MESH
    )
    plane = [y * 4 + xr, y * 4 + xl, yr * 4 + x, yl * 4 + x]
    for t in plane:
        pl.semaphore_signal(barrier, inc=1, device_id={"ep": ep, "tp": t}, device_id_type=MESH)

    def load(i, src, dst):
        cp = pltpu.make_async_copy(src, dst, loc.at[i])
        cp.start()
        return cp

    mid = pl.ds(WINDOW, LEN)
    rows_at = pl.ds(PACKED, TOK)
    ld_own = load(0, x_hbm, xg.at[y, x, rows_at])
    ld_route = [
        load(1, ids_hbm, ids_ref),
        load(2, rw_hbm, rw_ref),
        load(3, x_hbm, xpad.at[pl.ds(0, TOK)]),
    ]
    ld_kv = [load(4, k_hbm, kpad.at[mid]), load(5, v_hbm, vpad.at[mid])]
    def wait_all(copies):
        for cp in copies:
            cp.wait()

    late = {}

    def start_loads():
        ld_att = [
            load(6, q_hbm, q_ref),
            load(7, qg_hbm, qg_ref),
            load(8, kg_hbm, kg_ref),
            load(9, sink_hbm, sink_ref),
            load(10, colt_hbm, colt_ref),
            load(11, rowt_hbm.at[:, pl.ds(pl.multiple_of(ep * 8, 8), 16), :], rowt),
        ]
        ld_shared = [load(12, sg_hbm, sg_ref), load(13, su_hbm, su_ref), load(14, ng_hbm, ng_ref)] + [
            load(15 + j, sd_hbm, wsd.at[:, pl.ds(32 * j, 32), :]) for j in range(4)
        ]
        ld_big = [
            load(19, gate_hbm.at[0], wgu.at[:, 0:128]),
            load(20, up_hbm.at[0], wgu.at[:, 128:256]),
            load(21, down_hbm.at[0], wd),
        ]
        late.update(att=ld_att, shared=ld_shared, big=ld_big)

    xpad[TOK:TPAD, :] = jnp.zeros((TPAD - TOK, FEAT), BF)
    idsp[...] = jnp.full(idsp.shape, -1, jnp.int32)
    rwp[...] = jnp.zeros_like(rwp)
    wait_all(ld_route)
    idsp[0:TOP_K, 0:TOK] = ids_ref[...]
    rwp[0:TOP_K, 0:TOK] = rw_ref[...]

    row32 = lax.broadcasted_iota(jnp.int32, (32, TPAD), 0)
    pos32 = row32 >> 1
    rel32 = jnp.zeros((32, TPAD), jnp.int32)
    for p in range(NZ):
        rel32 = jnp.where(pos32 == p, REL[p] + NZ, rel32)
    expert32 = ((z + rel32) & (NZ - 1)) * 2 + (row32 & 1)
    named = jnp.zeros((32, TPAD), F32)
    weight = jnp.zeros((32, TPAD), F32)
    for k in range(TOP_K):
        same = idsp[k : k + 1, :] == expert32
        named = jnp.where(same, 1.0, named)
        weight = jnp.where(same, rwp[k : k + 1, :], weight)
    before = (
        lax.broadcasted_iota(jnp.int32, (TPAD, TPAD), 0)
        < lax.broadcasted_iota(jnp.int32, (TPAD, TPAD), 1)
    )
    count = jnp.dot(
        named.astype(BF), jnp.where(before, 1.0, 0.0).astype(BF), preferred_element_type=F32
    )
    slot32 = jnp.where(named > 0.5, count, -1.0)
    slot_row = lax.broadcasted_iota(jnp.int32, (SLOT, TPAD), 0).astype(F32)
    for t in range(NCHUNK):
        lo, n = ZFIRST[t], ZSIZE[t]
        picks = [
            jnp.where(slot32[i : i + 1, :] == slot_row, 1.0, 0.0).astype(BF)
            for i in range(lo // SLOT, (lo + n) // SLOT)
        ]
        send[lo : lo + n, :] = jnp.dot(
            jnp.concatenate(picks, axis=0), xpad[...], preferred_element_type=F32
        ).astype(BF)
    mine = pl.ds(pl.multiple_of(HERE * 2 * SLOT + core * SLOT, SLOT), SLOT)
    other = pl.ds(pl.multiple_of(HERE * 2 * SLOT + (1 - core) * SLOT, SLOT), SLOT)
    zst[mine, :] = send[mine, :]

    def moved(r):
        over = [jnp.where(r >= 30 * i, 2, 0) for i in (1, 2, 3)]
        return r + over[0] + over[1] + over[2]

    iota = lambda shape, axis: lax.broadcasted_iota(jnp.int32, shape, axis)
    wide_shape, tall_shape = (128, 128), (128, 128)
    pick[...] = jnp.where(
        moved(iota(wide_shape, 0)) == iota(wide_shape, 1), 1.0, 0.0
    ).astype(BF)
    spread[...] = jnp.where(
        iota(tall_shape, 0) == moved(iota(tall_shape, 1)), 1.0, 0.0
    ).astype(BF)

    def pack(c):
        rows = jnp.dot(
            pick[0 : SIZE[c], 0 : ZSIZE[c]],
            zst[ZFIRST[c] : ZFIRST[c] + ZSIZE[c], :],
            preferred_element_type=F32,
        )
        xg[y, x, FIRST[c] : FIRST[c] + SIZE[c], :] = rows.astype(BF)

    ld_own.wait()
    pl.semaphore_wait(barrier, 35)

    ends = []

    def remote(src, dst, ssem, rsem, dev):
        cp = pltpu.make_async_remote_copy(
            src_ref=src,
            dst_ref=dst,
            send_sem=ssem,
            recv_sem=rsem,
            device_id=dev,
            device_id_type=MESH,
        )
        return cp

    partner = {"ep": z * 2 + (1 - core), "tp": tp}

    class Gather:
        def __init__(self, which, buf, start, size, index):
            self.buf, self.width = buf, buf.shape[3]
            self.start, self.size = start, size
            self.index = which * NGATHER + index
            na = up8(size // 2)
            self.ranges = []
            for first, count in ((start, na), (start + na, size - na)):
                self.ranges.append((first, count, up8(count // 2)))
            self.stage = 0

        def next(self):
            s = self.stage
            self.stage += 1
            buf = self.buf
            ssem = g_send.at[self.index]
            if s > 0:
                rows = pl.ds(self.start, self.size)
                whole = (
                    buf.at[pl.ds(0, 2), 0, rows],
                    buf.at[0, 0, rows],
                    buf.at[pl.ds(0, 2), :, rows],
                    buf.at[0, :, rows],
                )[s - 1]
                rsem = g_recv.at[self.index * 3 + (s - 1) % 3]
                remote(whole, whole, ssem, rsem, partner).wait_recv()
            if s == 4:
                whole = lhs.at[pl.ds(0, 15), pl.ds(0, self.size), pl.ds(0, self.width)]
                ends.append(remote(whole, whole, ssem, g_recv.at[self.index * 3], partner))
                return
            near, wide = [], []
            for half, (first, count, low) in enumerate(self.ranges):
                full = pl.ds(first, count)
                part_lo, part_hi = pl.ds(first, low), pl.ds(first + low, count - low)
                if half == 0:
                    piece = lambda w, v, r: buf.at[w, v, r]
                    group = lambda w, r: buf.at[w, :, r]
                    n_me, n_r, n_l, n_o, w_me, w_r, w_l = x, xr, xl, xo, y, yr, yl
                    to_n, to_w = (y * 4 + xr, y * 4 + xl), (yr * 4 + x, yl * 4 + x)
                else:
                    piece = lambda w, v, r: buf.at[v, w, r]
                    group = lambda w, r: buf.at[:, w, r]
                    n_me, n_r, n_l, n_o, w_me, w_r, w_l = y, yr, yl, yo, x, xr, xl
                    to_n, to_w = (yr * 4 + x, yl * 4 + x), (y * 4 + xr, y * 4 + xl)
                if s == 0:
                    near += [(piece(w_me, n_me, full), to, 0) for to in to_n]
                    wide += [(piece(w_me, n_me, full), to, 2) for to in to_w]
                elif s == 1:
                    near += [
                        (piece(w_me, n_l, part_lo), to_n[0], 1),
                        (piece(w_me, n_r, part_hi), to_n[1], 1),
                    ]
                    wide += [(piece(w_me, v, full), to, 2) for v in (n_l, n_r) for to in to_w]
                elif s == 2:
                    wide += [(piece(w_me, n_o, full), to, 2) for to in to_w]
                else:
                    wide += [
                        (group(w_l, part_lo), to_w[0], 3),
                        (group(w_r, part_hi), to_w[1], 3),
                    ]
            for ref, to, kind in near + wide:
                remote(
                    ref, ref, ssem, g_recv.at[self.index * 3 + kind % 3], {"ep": ep, "tp": to}
                ).start()

    rows_g = [Gather(0, xg, s, n, i) for i, (s, n) in enumerate(GATHER_1)]
    hid_g = [Gather(1, hg, s, n, i) for i, (s, n) in enumerate(GATHER_2)]

    def z_start(chunk, src_at, dst_at, ssem, rsem):
        for p in range(ZFIRST[chunk] // (2 * SLOT), (ZFIRST[chunk] + ZSIZE[chunk]) // (2 * SLOT)):
            q = INV[p]
            back = pl.ds(pl.multiple_of(q * 2 * SLOT + core * SLOT, SLOT), SLOT)
            if REL[p] == 0:
                pieces = [(other, partner)]
            else:
                pieces = [
                    (
                        pl.ds(p * 2 * SLOT + c * SLOT, SLOT),
                        {"ep": ep_at(REL[p], c), "tp": tp},
                    )
                    for c in range(2)
                ]
            for rows, dev in pieces:
                remote(src_at(rows), dst_at(back), ssem.at[0], rsem.at[chunk], dev).start()

    def z_wait(chunk, at, rsem, ssem):
        rows = other if chunk == OWN_CHUNK else pl.ds(ZFIRST[chunk], ZSIZE[chunk])
        remote(at(rows), at(rows), ssem.at[0], rsem.at[chunk], partner).wait_recv()

    own_at = lambda r: zst.at[r]
    send_at = lambda r: send.at[r]
    res_at = lambda r: res.at[r]
    ret_at = lambda r: ret.at[r]

    def start_zin(chunk):
        z_start(chunk, send_at, own_at, zi_send, zi_recv)

    def wait_zin(chunk):
        z_wait(chunk, own_at, zi_recv, zi_send)
        pack(chunk)

    def start_zout(chunk):
        z_start(chunk, res_at, ret_at, zo_send, zo_recv)

    def wait_zout(chunk):
        z_wait(chunk, ret_at, zo_recv, zo_send)

    def start_halo():
        tail, head = pl.ds(LEN, WINDOW), pl.ds(WINDOW, WINDOW)
        wait_all(ld_kv)
        for i, pad in enumerate((kpad, vpad)):
            for j, (part, to, at) in enumerate(
                ((tail, ep_hi, pl.ds(0, WINDOW)), (head, ep_lo, pl.ds(WINDOW + LEN, WINDOW)))
            ):
                cp = remote(
                    pad.at[part],
                    pad.at[at],
                    halo_sem.at[0],
                    halo_sem.at[1],
                    {"ep": to, "tp": tp},
                )
                cp.start()
        ends.append(halo_all())

    def halo_all():
        ref = kpad.at[pl.ds(0, 4 * WINDOW)]
        return remote(ref, ref, halo_sem.at[0], halo_sem.at[1], partner)

    first_half = (lax.broadcasted_iota(jnp.int32, (GRID_W, HEAD_DIM), 1) & 63) < 32

    def turn(raw, gain, g):
        f = raw.astype(F32)
        n = f * lax.rsqrt(jnp.mean(f * f, axis=-1, keepdims=True) + EPS) * gain
        other = jnp.where(first_half, pltpu.roll(n, 96, 1), pltpu.roll(n, 32, 1))
        cos = rowt[0, pl.ds(g, 1), :] + colt_ref[0]
        sin = rowt[1, pl.ds(g, 1), :] + colt_ref[1]
        return (n * cos + other * sin).astype(BF)

    def turn_queries():
        for g in range(LEN // GRID_W):
            for h in range(2):
                rows = slice(g * GRID_W, (g + 1) * GRID_W)
                qt[h, rows, :] = turn(
                    q_ref[rows, h * HEAD_DIM : (h + 1) * HEAD_DIM], qg_ref[...], g + 2
                )

    def turn_keys():
        for g in range((LEN + 2 * WINDOW) // GRID_W):
            rows = slice(g * GRID_W, (g + 1) * GRID_W)
            kt[rows, :] = turn(kpad[rows, :], kg_ref[...], g)

    near_q = lax.broadcasted_iota(jnp.int32, (128, 384), 0)
    near_k = lax.broadcasted_iota(jnp.int32, (128, 384), 1)

    def attend(b):
        key_pos = near_k + (ep * LEN - WINDOW + 128 * b)
        inside = (
            (near_k >= near_q)
            & (near_k <= near_q + 2 * WINDOW)
            & (key_pos >= 0)
            & (key_pos < 32 * LEN)
        )
        keys = kt[128 * b : 128 * b + 384, :]
        values = vpad[128 * b : 128 * b + 384, :]
        for h in range(2):
            scores = lax.dot_general(
                qt[h, 128 * b : 128 * b + 128, :],
                keys,
                (((1,), (1,)), ((), ())),
                preferred_element_type=F32,
            ) * (HEAD_DIM ** (-0.5))
            raised = jnp.where(inside, jnp.exp(scores), 0.0)
            sink = jnp.exp(jnp.full((128, 1), sink_ref[h], F32))
            den = sink + jnp.sum(raised, axis=-1, keepdims=True)
            weights = (raised * (1.0 / den)).astype(BF)
            mixed = jnp.dot(weights, values, preferred_element_type=F32)
            att_ref[128 * b : 128 * b + 128, h * 128 : (h + 1) * 128] = mixed.astype(BF)

    def scale_rows(start, size):
        acc[0:size, 0:128] = jnp.zeros((size, 128), F32)

        def one(s, carry):
            f = xg[s // 4, s % 4, start : start + size, :].astype(F32)
            sq = f * f
            acc[0:size, 0:128] += sq[:, 0:128] + sq[:, 128:256]
            lhs[s, 0:size, :] = (f * ng_ref[:, pl.ds(pl.multiple_of(s * FEAT, FEAT), FEAT)]).astype(BF)
            return carry

        lax.fori_loop(0, 16, one, 0, unroll=4)
        return lax.rsqrt(jnp.sum(acc[0:size, 0:128], axis=-1, keepdims=True) / D + EPS)

    def activate(g, u, factor):
        g, u = g * factor, u * factor
        return (g / (1.0 + jnp.exp(-g)) * u).astype(BF)

    def experts_in(c):
        start, size = FIRST[c], SIZE[c]
        factor = scale_rows(start, size)
        both = jnp.dot(
            jnp.concatenate([lhs[s, 0:size, :] for s in range(16)], axis=1),
            wgu[...],
            preferred_element_type=F32,
        )
        hg[y, x, start : start + size, :] = activate(both[:, 0:128], both[:, 128:256], factor)

    def shared_in():
        factor = scale_rows(PACKED, TOK)
        rows = jnp.concatenate([lhs[s, 0:TOK, :] for s in range(16)], axis=1)
        across = (((1,), (1,)), ((), ()))
        g = lax.dot_general(rows, sg_ref[...], across, preferred_element_type=F32)
        u = lax.dot_general(rows, su_ref[...], across, preferred_element_type=F32)
        h = activate(g, u, factor).astype(F32)
        packed = jnp.concatenate([h[40 * j : 40 * j + 40, :] for j in range(4)], axis=1)
        hg[y, x, PACKED : PACKED + PACK, :] = packed.astype(BF)

    def experts_out(c):
        start, size = FIRST[c], SIZE[c]
        rows = jnp.concatenate(
            [hg[s // 4, s % 4, start : start + size, :] for s in range(16)], axis=1
        )
        packed = jnp.dot(rows, wd[...], preferred_element_type=F32).astype(BF)
        res[ZFIRST[c] : ZFIRST[c] + ZSIZE[c], :] = jnp.dot(
            spread[0 : ZSIZE[c], 0:size], packed, preferred_element_type=F32
        ).astype(BF)
        if c == OWN_CHUNK:
            ret[mine, :] = res[mine, :]

    def shared_out():
        group = lax.broadcasted_iota(jnp.int32, (40, 128), 1) // 32
        total = jnp.zeros((TOK, FEAT), F32)
        for s in range(16):
            piece = hg[s // 4, s % 4, PACKED : PACKED + PACK, :].astype(F32)[0:40, :]
            parts = jnp.concatenate(
                [jnp.where(group == j, piece, 0.0) for j in range(4)], axis=0
            )
            total += jnp.dot(parts.astype(BF), wsd[s], preferred_element_type=F32)
        sh_acc[...] = total

    def combine_weights():
        for t in range(ROWS // CHUNK):
            full = jnp.concatenate(
                [
                    jnp.where(slot32[i : i + 1, :] == slot_row, weight[i : i + 1, :], 0.0)
                    for i in range(8 * t, 8 * t + 8)
                ],
                axis=0,
            )
            turned = jnp.transpose(full)
            high = turned.astype(BF)
            rows = slice(t * CHUNK, (t + 1) * CHUNK)
            wt_hi[:, rows] = high
            wt_lo[:, rows] = (turned - high.astype(F32)).astype(BF)

    def combine(lo, hi):
        rows = ret[lo:hi, :]
        part = jnp.dot(wt_hi[:, lo:hi], rows, preferred_element_type=F32) + jnp.dot(
            wt_lo[:, lo:hi], rows, preferred_element_type=F32
        )
        sh_acc[...] += part[0:TOK, :]

    gathers = {f"R{c}": g for c, g in enumerate(rows_g)} | {f"H{c}": g for c, g in enumerate(hid_g)}

    def wait_halo():
        halo_all().wait_recv()

    def finish():
        most = pl.ds(0, ROWS - SLOT)
        ends.append(remote(send.at[most], send.at[most], zi_send.at[0], zi_recv.at[0], partner))
        ends.append(remote(res.at[most], res.at[most], zo_send.at[0], zo_recv.at[0], partner))
        out_ref[...] = sh_acc[...].astype(BF)
        for cp in ends:
            cp.wait_send()

    calls = dict(
        zi=start_zin,
        halo=start_halo,
        cw=combine_weights,
        tq=turn_queries,
        tk=turn_keys,
        wh=wait_halo,
        wi=wait_zin,
        zo=start_zout,
        wo=wait_zout,
        at=attend,
        si=shared_in,
        so=shared_out,
        ei=experts_in,
        eo=experts_out,
        cb=combine,
        go=start_loads,
        lda=lambda: wait_all(late["att"]),
        lds=lambda: wait_all(late["shared"]),
        ldb=lambda: wait_all(late["big"]),
        end=finish,
    )
    for item in ORDER:
        with jax.named_scope(item):
            if item in gathers:
                gathers[item].next()
            else:
                name, _, arg = item.partition(":")
                calls[name](*[int(v) for v in arg.split("-") if v])


def deliver(a_in, b_in, a_out, b_out, sems):
    copies = [
        pltpu.make_async_copy(a_in, a_out, sems.at[0]),
        pltpu.make_async_copy(b_in, b_out, sems.at[1]),
    ]
    for cp in copies:
        cp.start()
    for cp in copies:
        cp.wait()


def _tables():
    quarter = HEAD_DIM // 4
    freq = np.float32(ROTARY_BASE) ** (
        np.float32(-4.0) * np.arange(quarter, dtype=np.float32) / np.float32(HEAD_DIM)
    )
    freq = freq.astype(np.float32)
    sign = np.concatenate([-np.ones(quarter), np.ones(quarter)])

    def of(index):
        angle = (index.astype(np.float32)[:, None] * freq).astype(np.float32).astype(np.float64)
        angle = np.concatenate([angle, angle], axis=1)
        return np.cos(angle), np.sin(angle) * sign

    def put(pair, left):
        pads = [(0, 0), (0, 64)] if left else [(0, 0), (64, 0)]
        return np.stack([np.pad(v, pads) for v in pair]).astype(np.float32)

    rows = put(of(np.arange(-2, 270)), True)
    cols = put(of(np.arange(GRID_W)), False)
    return rows, cols


ROW_TABLE, COL_TABLE = _tables()


def shards(
    query_vectors,
    key_vectors,
    value_vectors,
    query_gain,
    key_gain,
    sink_logits,
    moe_rows,
    norm_gain,
    expert_ids,
    route_weights,
    expert_gate,
    expert_up,
    expert_down,
    shared_gate,
    shared_up,
    shared_down,
):
    vm = pl.BlockSpec(memory_space=pltpu.VMEM)
    hb = pl.BlockSpec(memory_space=pl.ANY)
    dma = pltpu.SemaphoreType.DMA
    made = pl.pallas_call(
        kernel,
        out_shape=(
            pltpu.VMEM((LEN, 2 * HEAD_DIM), BF),
            pltpu.VMEM((TOK, FEAT), BF),
        ),
        in_specs=[hb] * 18,
        out_specs=(vm, vm),
        scratch_shapes=[
            pltpu.VMEM((TOP_K, TOK), jnp.int32),
            pltpu.VMEM((TOP_K, TOK), F32),
            pltpu.VMEM((LEN, 2 * HEAD_DIM), BF),
            pltpu.VMEM((1, HEAD_DIM), F32),
            pltpu.VMEM((1, HEAD_DIM), F32),
            pltpu.SMEM((2,), F32),
            pltpu.VMEM((1, D), F32),
            pltpu.VMEM((2, GRID_W, HEAD_DIM), F32),
            pltpu.VMEM((32, D), BF),
            pltpu.VMEM((32, D), BF),
            pltpu.VMEM((4, 4, PACKED + TOK + 24, FEAT), BF),
            pltpu.VMEM((4, 4, PACKED + PACK + 16, UNITS), BF),
            pltpu.VMEM((D, 2 * UNITS), BF),
            pltpu.VMEM((16 * UNITS, FEAT), BF),
            pltpu.VMEM((16, 128, FEAT), BF),
            pltpu.VMEM((2, 16, 128), F32),
            pltpu.VMEM((LEN + 2 * WINDOW, HEAD_DIM), BF),
            pltpu.VMEM((LEN + 2 * WINDOW, HEAD_DIM), BF),
            pltpu.VMEM((2, LEN, HEAD_DIM), BF),
            pltpu.VMEM((LEN + 2 * WINDOW, HEAD_DIM), BF),
            pltpu.VMEM((TPAD, FEAT), BF),
            pltpu.VMEM((8, TPAD), jnp.int32),
            pltpu.VMEM((8, TPAD), F32),
            pltpu.VMEM((ROWS, FEAT), BF),
            pltpu.VMEM((TPAD, ROWS), BF),
            pltpu.VMEM((TPAD, ROWS), BF),
            pltpu.VMEM((16, CHUNK, FEAT), BF),
            pltpu.VMEM((ROWS, FEAT), BF),
            pltpu.VMEM((ROWS, FEAT), BF),
            pltpu.VMEM((CHUNK, 128), F32),
            pltpu.VMEM((TOK, FEAT), F32),
            pltpu.VMEM((ROWS, FEAT), BF),
            pltpu.VMEM((128, 128), BF),
            pltpu.VMEM((128, 128), BF),
            dma((2 * NGATHER,)),
            dma((6 * NGATHER,)),
            dma((1,)),
            dma((NCHUNK,)),
            dma((1,)),
            dma((NCHUNK,)),
            dma((2,)),
            dma((22,)),
        ],
        compiler_params=pltpu.CompilerParams(
            collective_id=0, has_side_effects=True, vmem_limit_bytes=66600000
        ),
        name="fused",
    )(
        moe_rows,
        expert_ids.T,
        route_weights.T,
        query_vectors,
        key_vectors,
        value_vectors,
        query_gain.reshape(1, HEAD_DIM),
        key_gain.reshape(1, HEAD_DIM),
        sink_logits,
        norm_gain.reshape(1, D),
        jnp.asarray(COL_TABLE),
        jnp.asarray(ROW_TABLE),
        expert_gate,
        expert_up,
        expert_down,
        shared_gate.T,
        shared_up.T,
        shared_down.reshape(16, 32, FEAT),
    )
    return pl.pallas_call(
        deliver,
        out_shape=tuple(jax.ShapeDtypeStruct(v.shape, v.dtype) for v in made),
        in_specs=[vm, vm],
        out_specs=(hb, hb),
        scratch_shapes=[dma((2,))],
        compiler_params=pltpu.CompilerParams(vmem_limit_bytes=2 * 1024 * 1024),
        name="deliver",
    )(*made)


def solution(mesh):
    placed = (
        P("ep", "tp"),
        P("ep", "tp"),
        P("ep", "tp"),
        P(),
        P(),
        P("tp"),
        P("ep", "tp"),
        P(),
        P("ep", None),
        P("ep", None),
        P("ep", None, "tp"),
        P("ep", None, "tp"),
        P("ep", None, "tp"),
        P(None, "tp"),
        P(None, "tp"),
        P(None, "tp"),
    )
    return jax.shard_map(
        shards,
        mesh=mesh,
        in_specs=placed,
        out_specs=(P("ep", "tp"), P("ep", "tp")),
        check_vma=False,
    )
```
